128 devices in a mesh: ep: 128 (over z, y, x, core).
Axes of the slice: x: 4, y: 4, z: 4, core: 2. Of those that a mesh axis runs over, the one named last changes fastest.
Arguments:
- tokens: bfloat16 [512, 2048], P('ep'), may hold values from -6 to 6
- lengths: int32 [512], P('ep'), may hold values from 1 to 1023
- cache_keys: bfloat16 [512, 1024, 2, 128], P('ep')
- cache_values: bfloat16 [512, 1024, 2, 128], P('ep'), may hold values from -6 to 6
- query_w: bfloat16 [2048, 1024], replicated, may hold values from -0.125 to 0.125
- key_w: bfloat16 [2048, 256], replicated, may hold values from -0.125 to 0.125
- value_w: bfloat16 [2048, 256], replicated, may hold values from -0.125 to 0.125
- out_w: bfloat16 [1024, 2048], replicated, may hold values from -0.1875 to 0.1875
- mix_lambda: float32 [8], replicated, may hold values from 0.3 to 0.8
- head_gain: float32 [128], replicated, may hold values from 0.1 to 1.9
- attn_gain: float32 [2048], replicated, may hold values from 0.1 to 1.9
- ffn_gain: float32 [2048], replicated, may hold values from 0.1 to 1.9
- routes: int32 [512, 2], P('ep'), may hold values from 0 to 7, all different within a row; in each aligned block of 4 rows (0 to 3, 4 to 7, ...) at most 2 rows name the same one
- route_weights: float32 [512, 2], P('ep'), may hold values from 0.2 to 1
- exp_gate: bfloat16 [2048, 49152], P(None, 'ep'), may hold values from -0.125 to 0.125
- exp_up: bfloat16 [2048, 49152], P(None, 'ep'), may hold values from -0.125 to 0.125
- exp_down: bfloat16 [49152, 2048], P('ep'), may hold values from -0.078125 to 0.078125
- dense_gate: bfloat16 [128, 256, 352], P('ep'), may hold values from -0.125 to 0.125
- dense_up: bfloat16 [128, 256, 352], P('ep'), may hold values from -0.125 to 0.125
- dense_down: bfloat16 [128, 352, 256], P('ep'), may hold values from -0.078125 to 0.078125
- branch_gate: bfloat16 [2048], replicated, may hold values from -0.125 to 0.125
Outputs:
- output: bfloat16 [512, 2048], P('ep')
- new_keys: bfloat16 [512, 256], P('ep')
- new_values: bfloat16 [512, 256], P('ep')
The draws below stay inside these ranges and needn't reach their ends.
Inputs may be any that keep to these rules, and one draw needn't show every extreme that they name: `routes`: each row names 2 different experts; among the 4 rows of one device no expert is named by more than 2 rows, a bound that some block reaches.
All inputs are finite; a program needn't handle non-finite values.
Results may differ from the reference program's by a relative error of at most 0.015.
Values may be sent and summed in bfloat16 or wider, within the bound.
No kernel may reach another device: no remote copies, remote signals or barrier semaphores. Data moves between devices by JAX's collectives and lax.ppermute only.
A program may use at most 128 MiB of HBM per device.

```python
import math
import jax
import jax.numpy as jnp
import numpy as np
from jax import lax

D = 2048
HEADS = 8
KV_HEADS = 2
HEAD_DIM = 128
CACHE = 1024
SEQ_DEV = 4
TOP_K = 2
SPLIT = 16
EXP_FF = 6144
DENSE_FF = 5632
EXPERTS = 8
BLOCKS = 8
CAP = 2
TOKENS = 512
N_EP = 128


def draw_cache_keys(key, part):
    shape = (TOKENS, CACHE, KV_HEADS, HEAD_DIM)
    base_key = jax.random.fold_in(jax.random.fold_in(key, 11), 0)
    values = jax.random.normal(base_key, shape, jnp.float32) * 1.75
    values = jnp.clip(values, -10.0, 10.0)
    return values.astype(jnp.bfloat16)


def plant(drawn, stream_key, least, high):
    longest = drawn.shape.index(max(drawn.shape))
    spots = []
    for shift in (0, 1):
        where = [jax.random.randint(jax.random.fold_in(stream_key, axis), (), 0, length) for axis, length in enumerate(drawn.shape)]
        where[longest] = (where[longest] + shift) % drawn.shape[longest]
        spots.append(tuple(where))
    return drawn.at[spots[0]].set(least).at[spots[1]].set(high)


def level_of(key, extent, cuts, low, top_value):
    level = 1.0
    for position, blocks in cuts:
        steps = jax.random.uniform(jax.random.fold_in(jax.random.fold_in(key, 6), position), (blocks,), jnp.float32, low / len(cuts), top_value / len(cuts))
        level = level * jnp.repeat(jnp.exp(steps), extent[position] // blocks).reshape((-1,) + (1,) * (len(extent) - 1 - position))
    return level


def deal_out(own_key, own, number, rows, number_of, top, most, lean):
    ranking = jax.random.permutation(own_key, number_of)
    packed, ordinary = load_shares(number_of, rows * top, most, lean, True), load_shares(number_of, rows * top, most, lean, False)
    places = jnp.arange(number_of)

    def named(sizes, offset_by):
        used = int((sizes > 0).sum())
        fixed = max(1, used // 4)
        passed = fixed + (places - fixed + offset_by * (used - fixed)) % max(1, number_of - fixed)
        return jnp.zeros((number_of,), jnp.int32).at[ranking[jnp.where(places < fixed, places, passed)]].set(jnp.asarray(sizes, jnp.int32))

    sizes = jnp.where(number % 4 == 0, named(packed, number // 4), named(ordinary, number - number // 4 - 1))
    mixed = jax.random.permutation(jax.random.fold_in(own, 3), number_of)
    source_of, receiver = mixed[0:number_of // 2 * 2:2], mixed[1:number_of // 2 * 2:2]
    slack = jnp.minimum(sizes[source_of] - 1, most - sizes[receiver]) // 2
    slack = jnp.where((source_of == ranking[0]) | (receiver == ranking[0]) | (sizes[receiver] == 0), 0, jnp.maximum(slack, 0))
    passed = jax.random.randint(jax.random.fold_in(own, 4), (number_of // 2,), 0, 1 << 20) % (slack + 1)
    sizes = sizes.at[source_of].add(-passed).at[receiver].add(passed)
    members = jnp.searchsorted(jnp.cumsum(sizes), jnp.arange(rows * top), side="right").astype(jnp.int32)
    listing = members.reshape(top, rows).T
    listing = listing[jax.random.permutation(jax.random.fold_in(own, 1), rows)]
    offset_by = jax.random.randint(jax.random.fold_in(own, 2), (rows, 1), 0, top)
    return jnp.take_along_axis(listing, (jnp.arange(top)[None, :] + offset_by) % top, axis=1)


def load_shares(count, total, limit, skew, full):
    loads = [(1 << 20) // math.isqrt(grade ** skew) + 1 for grade in range(1, count + 1)]
    largest = limit if full else min(limit, max(-(-total // count), total * loads[0] // sum(loads)))
    least = 1 if total - largest >= count - 1 else 0
    counts, spare = [largest] + [least] * (count - 1), total - largest - least * (count - 1)
    while spare > 0:
        free = [i for i in range(1, count) if counts[i] < largest] or [i for i in range(1, count) if counts[i] < limit]
        mass, left = sum([loads[i] for i in free]), spare
        for i in free:
            extra = min(limit - counts[i], max(1, left * loads[i] // mass), spare)
            counts[i] = counts[i] + extra
            spare = spare - extra
    return np.array(counts)


def centred(key, extent, spread, most, shards=(), kind=jnp.bfloat16):
    values = jax.random.normal(key, extent, jnp.float32) * spread
    if len(shards) > 0:
        values = level_of(key, extent, shards, -0.22, 0.18) * values
    return jnp.clip(values, min=-most, max=most).astype(kind)


def setup_inputs(seed: int = 0) -> dict:
    seeds = jax.random.split(jax.random.key(seed), 22)
    tokens = centred(seeds[0], (TOKENS, D), 1.0, 6.0, ((0, 128),))
    lengths = plant(jax.random.randint(seeds[1], (TOKENS,), 1, CACHE), jax.random.fold_in(seeds[1], 1), 1, CACHE - 1).astype(jnp.int32)
    cache_keys = draw_cache_keys(jax.random.fold_in(seeds[21], 71), 0)
    cache_values = centred(seeds[3], (TOKENS, CACHE, KV_HEADS, HEAD_DIM), 1.0, 6.0, ((0, 128),))
    query_w = centred(seeds[4], (D, HEADS * HEAD_DIM), D ** -0.5, 0.125)
    key_w = centred(seeds[5], (D, KV_HEADS * HEAD_DIM), D ** -0.5, 0.125)
    value_w = centred(seeds[6], (D, KV_HEADS * HEAD_DIM), D ** -0.5, 0.125)
    out_w = centred(seeds[7], (HEADS * HEAD_DIM, D), (HEADS * HEAD_DIM) ** -0.5, 0.1875)
    mix_lambda = jnp.clip(jax.random.uniform(seeds[8], (HEADS,), jnp.float32, 0.3, 0.8), 0.3, 0.8)
    head_gain = jnp.clip(1.0 + 0.18 * jax.random.normal(seeds[9], (HEAD_DIM,), jnp.float32), 0.1, 1.9)
    attn_gain = jnp.clip(1.0 + 0.18 * jax.random.normal(seeds[10], (D,), jnp.float32), 0.1, 1.9)
    ffn_gain = jnp.clip(1.0 + 0.18 * jax.random.normal(seeds[11], (D,), jnp.float32), 0.1, 1.9)
    routes_keys = jax.random.split(jax.random.fold_in(seeds[12], 1), TOKENS // SEQ_DEV)
    routes_turns = jax.random.permutation(jax.random.fold_in(seeds[12], 3), TOKENS // SEQ_DEV)
    routes = jax.vmap(lambda own, number: deal_out(jax.random.fold_in(seeds[12], 2), own, number, SEQ_DEV, EXPERTS, TOP_K, CAP, 1))(routes_keys, routes_turns).reshape((TOKENS, TOP_K))
    route_weights = jnp.clip(0.2 + 0.8 * jax.random.uniform(seeds[13], (TOKENS, TOP_K), jnp.float32) ** level_of(seeds[13], (TOKENS, TOP_K), ((0, 128),), -0.2, 0.2), 0.2, 1.0)
    exp_gate = centred(seeds[14], (D, EXPERTS * EXP_FF), D ** -0.5, 0.125, ((1, 128),))
    exp_up = centred(seeds[15], (D, EXPERTS * EXP_FF), D ** -0.5, 0.125, ((1, 128),))
    exp_down = centred(seeds[16], (EXPERTS * EXP_FF, D), EXP_FF ** -0.5, 0.078125, ((0, 128),))
    dense_gate = centred(seeds[17], (N_EP, D // BLOCKS, DENSE_FF // SPLIT), D ** -0.5, 0.125, ((0, 128),))
    dense_up = centred(seeds[18], (N_EP, D // BLOCKS, DENSE_FF // SPLIT), D ** -0.5, 0.125, ((0, 128),))
    dense_down = centred(seeds[19], (N_EP, DENSE_FF // SPLIT, D // BLOCKS), DENSE_FF ** -0.5, 0.078125, ((0, 128),))
    branch_gate = centred(seeds[20], (D,), D ** -0.5, 0.125)
    return {"tokens": tokens, "lengths": lengths, "cache_keys": cache_keys, "cache_values": cache_values, "query_w": query_w, "key_w": key_w, "value_w": value_w, "out_w": out_w, "mix_lambda": mix_lambda, "head_gain": head_gain, "attn_gain": attn_gain, "ffn_gain": ffn_gain, "routes": routes, "route_weights": route_weights, "exp_gate": exp_gate, "exp_up": exp_up, "exp_down": exp_down, "dense_gate": dense_gate, "dense_up": dense_up, "dense_down": dense_down, "branch_gate": branch_gate}


def rms_norm(values, gain, epsilon):
    scale = lax.rsqrt(lax.optimization_barrier(jnp.mean(values * values, axis=-1, keepdims=True)) + epsilon)
    return values * scale * gain.astype(jnp.float32)

def softmax_pair(scores, own_score, valid):
    masked = jnp.where(valid, scores, -jnp.inf)
    largest = jnp.maximum(lax.optimization_barrier(jnp.max(masked, axis=-1)), own_score)
    raised = jnp.where(valid, jnp.exp(scores - largest[..., None]), 0.0)
    own_raised = jnp.exp(own_score - largest)
    total = lax.optimization_barrier(jnp.sum(raised, axis=-1)) + own_raised
    return (raised / total[..., None], own_raised / total)

def attend_block(tokens, lengths, cache_keys, cache_values, query_w, key_w, value_w, out_w, mix_lambda, head_gain, attn_gain, ffn_gain):
    rows = tokens.shape[0]
    groups = HEADS // KV_HEADS
    half = HEAD_DIM // 2
    scale = (HEAD_DIM // 2) ** (-0.5)
    xfull = tokens.astype(jnp.float32)
    normed = rms_norm(xfull, attn_gain, 1e-06).astype(jnp.bfloat16)
    query = jnp.dot(normed, query_w, preferred_element_type=jnp.float32).astype(jnp.bfloat16)
    key_new = jnp.dot(normed, key_w, preferred_element_type=jnp.float32).astype(jnp.bfloat16)
    value_new = jnp.dot(normed, value_w, preferred_element_type=jnp.float32).astype(jnp.bfloat16)
    qfull = query.astype(jnp.float32).reshape(rows, KV_HEADS, groups, HEAD_DIM)
    knew = key_new.astype(jnp.float32).reshape(rows, KV_HEADS, HEAD_DIM)
    vnew = value_new.astype(jnp.float32).reshape(rows, KV_HEADS, HEAD_DIM)
    kcache = cache_keys.astype(jnp.float32)
    vcache = cache_values.astype(jnp.float32)
    valid = (jnp.arange(CACHE, dtype=jnp.int32)[None, :] < lengths[:, None])[:, None, None, :]
    first = jnp.einsum('sgqd,spgd->sgqp', qfull[..., :half], kcache[..., :half]) * scale
    first_own = jnp.einsum('sgqd,sgd->sgq', qfull[..., :half], knew[..., :half]) * scale
    second = jnp.einsum('sgqd,spgd->sgqp', qfull[..., half:], kcache[..., half:]) * scale
    second_own = jnp.einsum('sgqd,sgd->sgq', qfull[..., half:], knew[..., half:]) * scale
    prob_one, own_one = softmax_pair(first, first_own, valid)
    prob_two, own_two = softmax_pair(second, second_own, valid)
    lam = mix_lambda.astype(jnp.float32).reshape(KV_HEADS, groups)
    weights = (prob_one - lam[None, :, :, None] * prob_two).astype(jnp.bfloat16)
    own_weights = (own_one - lam[None] * own_two).astype(jnp.bfloat16)
    mixed = jnp.einsum('sgqp,spgd->sgqd', weights.astype(jnp.float32), vcache)
    mixed = mixed + own_weights.astype(jnp.float32)[..., None] * vnew[:, :, None, :]
    heads = rms_norm(mixed, head_gain, 1e-05).astype(jnp.bfloat16).reshape(rows, HEADS * HEAD_DIM)
    hidden_state = xfull + jnp.dot(heads, out_w, preferred_element_type=jnp.float32)
    ffn_in = rms_norm(hidden_state, ffn_gain, 1e-06).astype(jnp.bfloat16)
    return (hidden_state, ffn_in, key_new, value_new)

def reference(tokens, lengths, cache_keys, cache_values, query_w, key_w, value_w, out_w, mix_lambda, head_gain, attn_gain, ffn_gain, routes, route_weights, exp_gate, exp_up, exp_down, dense_gate, dense_up, dense_down, branch_gate):
    blocks = tokens.shape[0] // SEQ_DEV

    def one_block(pieces):
        return attend_block(pieces[0], pieces[1], pieces[2], pieces[3], query_w, key_w, value_w, out_w, mix_lambda, head_gain, attn_gain, ffn_gain)
    hidden_state, ffn_in, key_new, value_new = lax.map(one_block, (tokens.reshape(blocks, SEQ_DEV, D), lengths.reshape(blocks, SEQ_DEV), cache_keys.reshape(blocks, SEQ_DEV, CACHE, KV_HEADS, HEAD_DIM), cache_values.reshape(blocks, SEQ_DEV, CACHE, KV_HEADS, HEAD_DIM)))
    hidden_state = hidden_state.reshape(TOKENS, D)
    ffn_in = ffn_in.reshape(TOKENS, D)
    key_new = key_new.reshape(TOKENS, KV_HEADS * HEAD_DIM)
    value_new = value_new.reshape(TOKENS, KV_HEADS * HEAD_DIM)
    slots = N_EP * CAP

    def one_expert(total, expert):
        match = routes == expert
        hit = jnp.any(match, axis=-1)
        weight = lax.optimization_barrier(jnp.sum(jnp.where(match, route_weights.astype(jnp.float32), 0.0), axis=-1))
        rank = jnp.cumsum(hit.astype(jnp.int32)) - 1
        select = hit[None, :] & (rank[None, :] == jnp.arange(slots, dtype=jnp.int32)[:, None])
        chosen = jnp.dot(select.astype(jnp.bfloat16), ffn_in, preferred_element_type=jnp.float32).astype(jnp.bfloat16)
        start = (expert * EXP_FF).astype(jnp.int32)
        w_gate = lax.dynamic_slice_in_dim(exp_gate, start, EXP_FF, 1)
        w_up = lax.dynamic_slice_in_dim(exp_up, start, EXP_FF, 1)
        w_down = lax.dynamic_slice_in_dim(exp_down, start, EXP_FF, 0)
        gate_part = jnp.dot(chosen, w_gate, preferred_element_type=jnp.float32)
        up_part = jnp.dot(chosen, w_up, preferred_element_type=jnp.float32)
        act = (jax.nn.silu(gate_part) * up_part).astype(jnp.bfloat16)
        result = jnp.dot(act, w_down, preferred_element_type=jnp.float32)
        back = jnp.dot(select.astype(jnp.float32).T, result, precision=lax.Precision.HIGHEST)
        return (total + weight[:, None] * back, None)
    routed, unused = lax.scan(one_expert, jnp.zeros((TOKENS, D), jnp.float32), jnp.arange(EXPERTS, dtype=jnp.int32))
    row_span = D // BLOCKS
    col_span = DENSE_FF // SPLIT
    gate_full = dense_gate.reshape(BLOCKS, SPLIT, row_span, col_span).transpose(0, 2, 1, 3).reshape(D, DENSE_FF)
    up_full = dense_up.reshape(BLOCKS, SPLIT, row_span, col_span).transpose(0, 2, 1, 3).reshape(D, DENSE_FF)
    down_full = dense_down.reshape(BLOCKS, SPLIT, col_span, row_span).transpose(1, 2, 0, 3).reshape(DENSE_FF, D)
    gate_part = jnp.dot(ffn_in, gate_full, preferred_element_type=jnp.float32)
    up_part = jnp.dot(ffn_in, up_full, preferred_element_type=jnp.float32)
    dense_act = (jax.nn.silu(gate_part) * up_part).astype(jnp.bfloat16)
    dense = jnp.dot(dense_act, down_full, preferred_element_type=jnp.float32)
    gate = jax.nn.sigmoid(jnp.dot(ffn_in, branch_gate, preferred_element_type=jnp.float32))
    output = (hidden_state + routed + gate[:, None] * dense).astype(jnp.bfloat16)
    return (output, key_new, value_new)
```

```python
import jax
import jax.numpy as jnp
from jax import lax
from jax.experimental import pallas as pl
from jax.experimental.pallas import tpu as pltpu
from jax.sharding import PartitionSpec as P

HEADS = 8
KV_HEADS = 2
HEAD_DIM = 128
DEVICES = 128
D = 2048
HALF = D // 2
UNITS = 48
PIECE = 3 * UNITS
TAIL = 128
WIDTH = 384
STRIDE = {"z": 32, "y": 8, "x": 2}
ORDERS = (("x", "y", "z"), ("y", "z", "x"), ("z", "x", "y"))
WIDTHS = (384, 384, 256)
f32 = jnp.float32
bf16 = jnp.bfloat16


def moved(index, shift):
    out = index
    for name, steps in shift.items():
        if name == "core":
            out = out ^ steps
            continue
        stride = STRIDE[name]
        place = index // stride % 4
        out += ((place + steps) % 4 - place) * stride
    return out


def send(x, shift):
    return lax.ppermute(x, "ep", [(i, moved(i, shift)) for i in range(DEVICES)])


def fetch(x, name, steps):
    return send(x, {name: -steps})


def rms_norm(values, gain, epsilon):
    scale = lax.rsqrt(jnp.mean(values * values, axis=-1, keepdims=True) + epsilon)
    return values * scale * gain


def softmax_pair(scores, own_score, valid):
    masked = jnp.where(valid, scores, -jnp.inf)
    largest = jnp.maximum(jnp.max(masked, axis=-1), own_score)
    raised = jnp.where(valid, jnp.exp(scores - largest[..., None]), 0.0)
    own_raised = jnp.exp(own_score - largest)
    total = jnp.sum(raised, axis=-1) + own_raised
    return (raised / total[..., None], own_raised / total)


def attend(tokens, lengths, cache_keys, cache_values, query_w, key_w, value_w, out_w, mix_lambda, head_gain, attn_gain, ffn_gain):
    rows = tokens.shape[0]
    groups = HEADS // KV_HEADS
    half = HEAD_DIM // 2
    scale = half ** (-0.5)
    cache_len = cache_keys.shape[1]
    xfull = tokens.astype(f32)
    normed = rms_norm(xfull, attn_gain, 1e-06).astype(bf16)
    query = jnp.dot(normed, query_w, preferred_element_type=f32).astype(bf16)
    key_new = jnp.dot(normed, key_w, preferred_element_type=f32).astype(bf16)
    value_new = jnp.dot(normed, value_w, preferred_element_type=f32).astype(bf16)
    qheads = query.reshape(rows, KV_HEADS, groups, HEAD_DIM)
    knew = key_new.reshape(rows, KV_HEADS, HEAD_DIM)
    vnew = value_new.reshape(rows, KV_HEADS, HEAD_DIM)
    valid = (jnp.arange(cache_len, dtype=jnp.int32)[None, :] < lengths[:, None])[:, None, None, :]
    probs = []
    for lo in (0, half):
        part = slice(lo, lo + half)
        scores = jnp.einsum("sgqd,spgd->sgqp", qheads[..., part], cache_keys[..., part], preferred_element_type=f32) * scale
        own = jnp.einsum("sgqd,sgd->sgq", qheads[..., part], knew[..., part], preferred_element_type=f32) * scale
        probs.append(softmax_pair(scores, own, valid))
    (prob_one, own_one), (prob_two, own_two) = probs
    lam = mix_lambda.reshape(KV_HEADS, groups)
    weights = (prob_one - lam[None, :, :, None] * prob_two).astype(bf16)
    own_weights = (own_one - lam[None] * own_two).astype(bf16)
    mixed = jnp.einsum("sgqp,spgd->sgqd", weights, cache_values, preferred_element_type=f32)
    mixed = mixed + own_weights.astype(f32)[..., None] * vnew.astype(f32)[:, :, None, :]
    heads = rms_norm(mixed, head_gain, 1e-05).astype(bf16).reshape(rows, HEADS * HEAD_DIM)
    hidden_state = xfull + jnp.dot(heads, out_w, preferred_element_type=f32)
    ffn_in = rms_norm(hidden_state, ffn_gain, 1e-06).astype(bf16)
    return hidden_state, ffn_in, key_new, value_new


def pieces_kernel(ids, gate, up, down, *refs):
    outs, held = refs[:8], refs[8]
    z, high = ids[2], ids[3]
    held[:, 352:384, :] = jnp.zeros((3, 32, 256), bf16)
    held[0, 0:352, :] = gate[...]
    held[1, 0:352, :] = up[...]
    held[2, 0:352, :] = down[...]
    for k in range(8):
        block = 2 * lax.rem(z + k // 2, 4) + lax.rem(high + k % 2, 2)
        start = pl.multiple_of(block * UNITS, 16)
        for m in range(3):
            outs[k][m * UNITS : (m + 1) * UNITS, :] = held[m, pl.ds(start, UNITS), :]


def dot(a, b):
    return jnp.dot(a, b, preferred_element_type=f32)


def place_of(part, slab, block):
    a, b, c = ORDERS[part]
    where = {a: block % 4, b: block // 4, c: slab}
    return where["z"] * 16 + where["y"] * 4 + where["x"]


def ffn_kernel(ids, *refs):
    slabs = refs[:24]
    pieces = refs[24:32]
    w_gate, w_up, w_down, branch = refs[32:36]
    y_other, y_own = refs[36:38]
    rows, near, far = refs[38:41]
    core, expert, z, high = ids[0], ids[1], ids[2], ids[3]
    for side in range(2):
        for part in range(3):
            for slab in range(4):
                ref = slabs[side * 12 + part * 4 + slab]
                for block in range(16):
                    spot = place_of(part, slab, block)
                    rows[side, spot * 8 : spot * 8 + 8, part * WIDTH : (part + 1) * WIDTH] = ref[block * 8 : block * 8 + 8, :]
    near[...] = jnp.zeros_like(near)
    far[...] = jnp.zeros_like(far)
    for k in range(8):
        block = 2 * lax.rem(z + 4 - k // 2, 4) + lax.rem(high + k % 2, 2)
        near[block, 0:UNITS, :] = pieces[k][0:UNITS, :]
        near[block, 128 : 128 + UNITS, :] = pieces[k][UNITS : 2 * UNITS, :]
        far[0:UNITS, pl.ds(pl.multiple_of(block * 256, 256), 256)] = pieces[k][2 * UNITS :, :]
    for b in range(8):
        near[b, 64:72, :] = jnp.broadcast_to(branch[:, b * 256 : (b + 1) * 256], (8, 256))
    halves = (core, 1 - core)
    gate_sum = up_sum = both = None
    for side in range(2):
        base = pl.multiple_of(halves[side] * HALF, HALF)
        x = rows[side, :, 0:HALF]
        gate_part = dot(x, w_gate[pl.ds(base, HALF), :])
        up_part = dot(x, w_up[pl.ds(base, HALF), :])
        gate_sum = gate_part if side == 0 else gate_sum + gate_part
        up_sum = up_part if side == 0 else up_sum + up_part
        for j in range(4):
            xj = rows[side, :, j * 256 : (j + 1) * 256]
            term = lax.dot_general(xj, near[halves[side] * 4 + j], (((1,), (1,)), ((), ())), preferred_element_type=f32)
            both = term if both is None else both + term
    act = (gate_sum * jax.nn.sigmoid(gate_sum) * up_sum).astype(bf16)
    dense_gate = both[:, 0:128]
    dense_act = (dense_gate * jax.nn.sigmoid(dense_gate) * both[:, 128:256]).astype(bf16)
    lane = lax.broadcasted_iota(jnp.int32, (512, 128), 1)
    gate = jax.nn.sigmoid(jnp.sum(jnp.where(lane == 64, dense_gate, 0.0), axis=1, keepdims=True))
    tail = rows[0, :, HALF : HALF + TAIL].astype(f32)
    weight = jnp.sum(jnp.where((lane == expert) | (lane == expert + 8), tail, 0.0), axis=1, keepdims=True)
    lane48 = lane < UNITS
    dense_act = jnp.where(lane48, dense_act.astype(f32), 0.0).astype(bf16)
    for side, ref in ((1, y_other), (0, y_own)):
        base = pl.multiple_of(halves[side] * HALF, HALF)
        total = weight * dot(act, w_down[:, pl.ds(base, HALF)]) + gate * dot(dense_act, far[:, pl.ds(base, HALF)])
        ref[...] = total.astype(ref.dtype)


def split_kernel(y_own, y_recv, *outs):
    at = 0
    for part in range(3):
        width = WIDTHS[part]
        for slab in range(4):
            for block in range(16):
                spot = place_of(part, slab, block)
                rows = slice(spot * 8, spot * 8 + 8)
                total = y_own[rows, at : at + width] + y_recv[rows, at : at + width].astype(f32)
                outs[part * 4 + slab][block * 8 : block * 8 + 8, :] = total.astype(bf16)
        at += width


def sum_kernel(*refs):
    ins, outs = refs[:12], refs[12:]
    for part in range(3):
        total = ins[part * 4][...].astype(f32)
        for k in range(1, 4):
            total = total + ins[part * 4 + k][...].astype(f32)
        size = total.shape[0] // 4
        for k in range(4):
            outs[part * 4 + k][...] = total[k * size : (k + 1) * size, :].astype(bf16)


def last_kernel(*refs):
    ins, out = refs[:12], refs[12]
    at = 0
    for part in range(3):
        total = ins[part * 4][...].astype(f32)
        for k in range(1, 4):
            total = total + ins[part * 4 + k][...].astype(f32)
        out[:, at : at + WIDTHS[part]] = total
        at += WIDTHS[part]


def call(kernel, outs, operands, scratch=(), ids=None):
    vmem = pl.BlockSpec(memory_space=pltpu.VMEM)
    specs = [vmem] * len(operands)
    if ids is not None:
        specs = [pl.BlockSpec(memory_space=pltpu.SMEM)] + specs
        operands = [ids] + list(operands)
    return pl.pallas_call(
        kernel,
        in_specs=specs,
        out_specs=[vmem] * len(outs),
        out_shape=[jax.ShapeDtypeStruct(s, d) for s, d in outs],
        scratch_shapes=list(scratch),
        compiler_params=pltpu.CompilerParams(vmem_limit_bytes=40 * 1024 * 1024),
        name=kernel.__name__,
    )(*operands)


def per_device(
    tokens, lengths, cache_keys, cache_values, query_w, key_w, value_w, out_w, mix_lambda, head_gain, attn_gain, ffn_gain,
    routes, route_weights, exp_gate, exp_up, exp_down, dense_gate, dense_up, dense_down, branch_gate,
):
    rows = tokens.shape[0]
    me = lax.axis_index("ep")
    core = me % 2
    ids = jnp.stack([core, me // 16, me // 32, me // 16 % 2]).astype(jnp.int32)

    pieces = call(
        pieces_kernel,
        [((PIECE, 256), bf16)] * 8,
        [jnp.swapaxes(dense_gate[0], 0, 1), jnp.swapaxes(dense_up[0], 0, 1), dense_down[0]],
        [pltpu.VMEM((3, 384, 256), bf16)],
        ids,
    )
    pieces = [pieces[0]] + [send(pieces[k], {"z": k // 2, "y": 2 * (k % 2)}) for k in range(1, 8)]

    hidden_state, ffn_in, key_new, value_new = attend(
        tokens, lengths, cache_keys, cache_values, query_w, key_w, value_w, out_w, mix_lambda, head_gain, attn_gain, ffn_gain
    )

    spread = jnp.sum(jnp.where(routes[:, :, None] == jnp.arange(8, dtype=jnp.int32), route_weights[:, :, None], 0.0), axis=1)
    upper = lax.reduce_precision(spread, 8, 7)
    tail = jnp.concatenate([upper, spread - upper, jnp.zeros((rows, TAIL - 16), f32)], axis=1).astype(bf16)
    low, high = ffn_in[:, :HALF], ffn_in[:, HALF:]
    mine = jnp.concatenate([jnp.where(core == 0, low, high), tail], axis=1)
    other = jnp.concatenate([jnp.where(core == 0, high, low), tail], axis=1)
    theirs = send(other, {"core": 1})
    chip = jnp.where(core == 0, jnp.concatenate([mine, theirs]), jnp.concatenate([theirs, mine]))
    slabs = []
    for part in range(3):
        a, b, c = ORDERS[part]
        block = chip[:, part * WIDTH : (part + 1) * WIDTH]
        for name in (a, b):
            block = jnp.concatenate([block] + [fetch(block, name, k) for k in (1, 2, 3)])
        slabs += [block] + [fetch(block, c, k) for k in (1, 2, 3)]
    slabs += [send(x, {"core": 1}) for x in slabs]

    y_other, y_own = call(
        ffn_kernel,
        [((512, HALF), bf16), ((512, HALF), f32)],
        slabs + pieces + [exp_gate, exp_up, exp_down, branch_gate.reshape(1, D)],
        [pltpu.VMEM((2, 512, 3 * WIDTH), bf16), pltpu.VMEM((8, 256, 256), bf16), pltpu.VMEM((128, D), bf16)],
        ids,
    )
    y_recv = send(y_other, {"core": 1})
    parts = call(split_kernel, [((128, w), bf16) for w in WIDTHS for _ in range(4)], [y_own, y_recv])
    for stage in (2, 1, 0):
        parts = [
            parts[part * 4 + k] if k == 0 else send(parts[part * 4 + k], {ORDERS[part][stage]: k}) for part in range(3) for k in range(4)
        ]
        if stage:
            size = 32 if stage == 2 else 8
            parts = call(sum_kernel, [((size, w), bf16) for w in WIDTHS for _ in range(4)], parts)
    (total,) = call(last_kernel, [((8, HALF), f32)], parts)
    keep = jnp.where(core == 0, total[:4], total[4:])
    give = jnp.where(core == 0, total[4:], total[:4])
    got = send(give, {"core": 1})
    added = jnp.where(core == 0, jnp.concatenate([keep, got], axis=1), jnp.concatenate([got, keep], axis=1))
    output = (hidden_state + added).astype(bf16)
    return (output, key_new, value_new)


def solution(mesh):
    placed = (
        P("ep", None),
        P("ep"),
        P("ep", None, None, None),
        P("ep", None, None, None),
        P(),
        P(),
        P(),
        P(),
        P(),
        P(),
        P(),
        P(),
        P("ep", None),
        P("ep", None),
        P(None, "ep"),
        P(None, "ep"),
        P("ep", None),
        P("ep", None, None),
        P("ep", None, None),
        P("ep", None, None),
        P(),
    )
    return jax.shard_map(
        per_device,
        mesh=mesh,
        in_specs=placed,
        out_specs=(P("ep", None), P("ep", None), P("ep", None)),
        check_vma=False,
    )
```

```python
import jax
import jax.numpy as jnp
from jax import lax
from jax.experimental import pallas as pl
from jax.experimental.pallas import tpu as pltpu
from jax.sharding import PartitionSpec as P

HEADS = 8
KV_HEADS = 2
HEAD_DIM = 128
DEVICES = 128
D = 2048
HALF = D // 2
UNITS = 48
PIECE = 3 * UNITS
TAIL = 128
f32 = jnp.float32
bf16 = jnp.bfloat16

def to_partner(x):
    return lax.ppermute(x, "ep", [(i, i ^ 1) for i in range(DEVICES)])


def rms_norm(values, gain, epsilon):
    scale = lax.rsqrt(jnp.mean(values * values, axis=-1, keepdims=True) + epsilon)
    return values * scale * gain


def softmax_pair(scores, own_score, valid):
    masked = jnp.where(valid, scores, -jnp.inf)
    largest = jnp.maximum(jnp.max(masked, axis=-1), own_score)
    raised = jnp.where(valid, jnp.exp(scores - largest[..., None]), 0.0)
    own_raised = jnp.exp(own_score - largest)
    total = jnp.sum(raised, axis=-1) + own_raised
    return (raised / total[..., None], own_raised / total)


def attend(tokens, lengths, cache_keys, cache_values, query_w, key_w, value_w, out_w, mix_lambda, head_gain, attn_gain, ffn_gain):
    rows = tokens.shape[0]
    groups = HEADS // KV_HEADS
    half = HEAD_DIM // 2
    scale = half ** (-0.5)
    cache_len = cache_keys.shape[1]
    xfull = tokens.astype(f32)
    normed = rms_norm(xfull, attn_gain, 1e-06).astype(bf16)
    query = jnp.dot(normed, query_w, preferred_element_type=f32).astype(bf16)
    key_new = jnp.dot(normed, key_w, preferred_element_type=f32).astype(bf16)
    value_new = jnp.dot(normed, value_w, preferred_element_type=f32).astype(bf16)
    qheads = query.reshape(rows, KV_HEADS, groups, HEAD_DIM)
    knew = key_new.reshape(rows, KV_HEADS, HEAD_DIM)
    vnew = value_new.reshape(rows, KV_HEADS, HEAD_DIM)
    valid = (jnp.arange(cache_len, dtype=jnp.int32)[None, :] < lengths[:, None])[:, None, None, :]
    probs = []
    for lo in (0, half):
        part = slice(lo, lo + half)
        scores = jnp.einsum("sgqd,spgd->sgqp", qheads[..., part], cache_keys[..., part], preferred_element_type=f32) * scale
        own = jnp.einsum("sgqd,sgd->sgq", qheads[..., part], knew[..., part], preferred_element_type=f32) * scale
        probs.append(softmax_pair(scores, own, valid))
    (prob_one, own_one), (prob_two, own_two) = probs
    lam = mix_lambda.reshape(KV_HEADS, groups)
    weights = (prob_one - lam[None, :, :, None] * prob_two).astype(bf16)
    own_weights = (own_one - lam[None] * own_two).astype(bf16)
    mixed = jnp.einsum("sgqp,spgd->sgqd", weights, cache_values, preferred_element_type=f32)
    mixed = mixed + own_weights.astype(f32)[..., None] * vnew.astype(f32)[:, :, None, :]
    heads = rms_norm(mixed, head_gain, 1e-05).astype(bf16).reshape(rows, HEADS * HEAD_DIM)
    hidden_state = xfull + jnp.dot(heads, out_w, preferred_element_type=f32)
    ffn_in = rms_norm(hidden_state, ffn_gain, 1e-06).astype(bf16)
    return hidden_state, ffn_in, key_new, value_new


def pieces_kernel(gate, up, down, out):
    for m, ref in enumerate((gate, up, down)):
        for k in range(8):
            size = min(UNITS, ref.shape[0] - k * UNITS)
            out[k, m * UNITS : m * UNITS + size, :] = ref[k * UNITS : k * UNITS + size, :]
            if size < UNITS:
                out[k, m * UNITS + size : (m + 1) * UNITS, :] = jnp.zeros((UNITS - size, 256), bf16)


def dot(a, b):
    return jnp.dot(a, b, preferred_element_type=f32)


def ffn_kernel(ids, own, theirs, pieces, w_gate, w_up, w_down, branch, y_other, y_own, rows, near, far):
    core, expert = ids[0], ids[1]
    for side, ref in enumerate((own, theirs)):
        rows[side] = ref[...].reshape(512, HALF + TAIL)
    near[...] = jnp.zeros_like(near)
    far[...] = jnp.zeros_like(far)
    for b in range(8):
        near[b, 0:UNITS, :] = pieces[b, 0:UNITS, :]
        near[b, 128 : 128 + UNITS, :] = pieces[b, UNITS : 2 * UNITS, :]
        near[b, 64:72, :] = jnp.broadcast_to(branch[:, b * 256 : (b + 1) * 256], (8, 256))
        far[0:UNITS, b * 256 : (b + 1) * 256] = pieces[b, 2 * UNITS :, :]
    halves = (core, 1 - core)
    gate_sum = up_sum = both = None
    for side in range(2):
        base = pl.multiple_of(halves[side] * HALF, HALF)
        x = rows[side, :, 0:HALF]
        gate_part = dot(x, w_gate[pl.ds(base, HALF), :])
        up_part = dot(x, w_up[pl.ds(base, HALF), :])
        gate_sum = gate_part if side == 0 else gate_sum + gate_part
        up_sum = up_part if side == 0 else up_sum + up_part
        for j in range(4):
            xj = rows[side, :, j * 256 : (j + 1) * 256]
            term = lax.dot_general(xj, near[halves[side] * 4 + j], (((1,), (1,)), ((), ())), preferred_element_type=f32)
            both = term if both is None else both + term
    act = (gate_sum * jax.nn.sigmoid(gate_sum) * up_sum).astype(bf16)
    dense_gate = both[:, 0:128]
    dense_act = dense_gate * jax.nn.sigmoid(dense_gate) * both[:, 128:256]
    lane = lax.broadcasted_iota(jnp.int32, (512, 128), 1)
    gate = jax.nn.sigmoid(jnp.sum(jnp.where(lane == 64, dense_gate, 0.0), axis=1, keepdims=True))
    tail = rows[0, :, HALF : HALF + TAIL].astype(f32)
    weight = jnp.sum(jnp.where((lane == expert) | (lane == expert + 8), tail, 0.0), axis=1, keepdims=True)
    dense_act = jnp.where(lane < UNITS, dense_act, 0.0).astype(bf16)
    for side, ref in ((1, y_other), (0, y_own)):
        base = pl.multiple_of(halves[side] * HALF, HALF)
        total = weight * dot(act, w_down[:, pl.ds(base, HALF)]) + gate * dot(dense_act, far[:, pl.ds(base, HALF)])
        ref[...] = total.astype(ref.dtype)


def join_kernel(y_own, y_recv, out):
    out[...] = (y_own[...] + y_recv[...].astype(f32)).astype(bf16).reshape(128, 4, HALF)


def last_kernel(hidden, parts, out):
    for half in range(2):
        total = jnp.zeros((4, HALF), f32)
        for chip in range(64):
            total = total + parts[2 * chip + half].astype(f32)
        cols = slice(half * HALF, (half + 1) * HALF)
        out[:, cols] = (hidden[:, cols] + total).astype(bf16)


def call(kernel, outs, operands, scratch=(), ids=None):
    vmem = pl.BlockSpec(memory_space=pltpu.VMEM)
    specs = [vmem] * len(operands)
    if ids is not None:
        specs = [pl.BlockSpec(memory_space=pltpu.SMEM)] + specs
        operands = [ids] + list(operands)
    return pl.pallas_call(
        kernel,
        in_specs=specs,
        out_specs=[vmem] * len(outs),
        out_shape=[jax.ShapeDtypeStruct(s, d) for s, d in outs],
        scratch_shapes=list(scratch),
        compiler_params=pltpu.CompilerParams(vmem_limit_bytes=40 * 1024 * 1024),
        name=kernel.__name__,
    )(*operands)


def per_device(
    tokens, lengths, cache_keys, cache_values, query_w, key_w, value_w, out_w, mix_lambda, head_gain, attn_gain, ffn_gain,
    routes, route_weights, exp_gate, exp_up, exp_down, dense_gate, dense_up, dense_down, branch_gate,
):
    rows = tokens.shape[0]
    me = lax.axis_index("ep")
    core = me % 2
    ids = jnp.stack([core, me // 16]).astype(jnp.int32)

    (pieces,) = call(
        pieces_kernel,
        [((8, PIECE, 256), bf16)],
        [jnp.swapaxes(dense_gate[0], 0, 1), jnp.swapaxes(dense_up[0], 0, 1), dense_down[0]],
    )
    columns = [[16 * b + j for b in range(8)] for j in range(16)]
    pieces = lax.all_to_all(pieces, "ep", 0, 0, axis_index_groups=columns, tiled=True)

    hidden_state, ffn_in, key_new, value_new = attend(
        tokens, lengths, cache_keys, cache_values, query_w, key_w, value_w, out_w, mix_lambda, head_gain, attn_gain, ffn_gain
    )

    spread = jnp.sum(jnp.where(routes[:, :, None] == jnp.arange(8, dtype=jnp.int32), route_weights[:, :, None], 0.0), axis=1)
    upper = lax.reduce_precision(spread, 8, 7)
    tail = jnp.concatenate([upper, spread - upper, jnp.zeros((rows, TAIL - 16), f32)], axis=1).astype(bf16)
    pair = jnp.stack([jnp.concatenate([ffn_in[:, :HALF], tail], axis=1), jnp.concatenate([ffn_in[:, HALF:], tail], axis=1)])
    outgoing = jnp.broadcast_to(pair[None], (64, 2, rows, HALF + TAIL)).reshape(DEVICES, rows, HALF + TAIL)
    own = lax.all_to_all(outgoing, "ep", 0, 0, tiled=True)
    theirs = to_partner(own)
    y_other, y_own = call(
        ffn_kernel,
        [((512, HALF), bf16), ((512, HALF), f32)],
        [own, theirs, pieces, exp_gate, exp_up, exp_down, branch_gate.reshape(1, D)],
        [pltpu.VMEM((2, 512, HALF + TAIL), bf16), pltpu.VMEM((8, 256, 256), bf16), pltpu.VMEM((128, D), bf16)],
        ids,
    )
    y_recv = to_partner(y_other)
    (joined,) = call(join_kernel, [((DEVICES, rows, HALF), bf16)], [y_own, y_recv])
    parts = lax.all_to_all(joined, "ep", 0, 0, tiled=True)
    (output,) = call(last_kernel, [((rows, D), bf16)], [hidden_state, parts])
    return (output, key_new, value_new)


def solution(mesh):
    placed = (
        P("ep", None),
        P("ep"),
        P("ep", None, None, None),
        P("ep", None, None, None),
        P(),
        P(),
        P(),
        P(),
        P(),
        P(),
        P(),
        P(),
        P("ep", None),
        P("ep", None),
        P(None, "ep"),
        P(None, "ep"),
        P("ep", None),
        P("ep", None, None),
        P("ep", None, None),
        P("ep", None, None),
        P(),
    )
    return jax.shard_map(
        per_device,
        mesh=mesh,
        in_specs=placed,
        out_specs=(P("ep", None), P("ep", None), P("ep", None)),
        check_vma=False,
    )
```

```python
import jax
import jax.numpy as jnp
from jax import lax
from jax.experimental import pallas as pl
from jax.experimental.pallas import tpu as pltpu
from jax.sharding import PartitionSpec as P


HEADS = 8
KV_HEADS = 2
HEAD_DIM = 128
DEVICES = 128
D = 2048
HALF = D // 2
UNITS = 48
PIECE = 3 * UNITS
TAIL = 128
f32 = jnp.float32
bf16 = jnp.bfloat16


def to_partner(x):
    return lax.ppermute(x, "ep", [(i, i ^ 1) for i in range(DEVICES)])


def rms_norm(values, gain, epsilon):
    scale = lax.rsqrt(jnp.mean(values * values, axis=-1, keepdims=True) + epsilon)
    return values * scale * gain


def dot_last(a, b):
    return lax.dot_general(a, b, (((1,), (1,)), ((), ())), preferred_element_type=f32)


def attend_kernel(
    lengths, routes, route_weights, tokens, mix_lambda, head_gain, attn_gain, ffn_gain,
    query_hbm, key_hbm, value_hbm, cache_keys, cache_values, out_hbm, gate_hbm, up_hbm, down_hbm,
    pair, hidden, key_new, value_new, w_gate, w_up, w_down,
    query_w, key_w, value_w, keys, values, out_w, sem, query_rows, head_rows,
):
    span = keys.shape[0] // 4
    copies = []

    def fetch(source, target):
        copies.append(pltpu.make_async_copy(source, target, sem.at[len(copies)]))
        copies[-1].start()
        return copies[-1]

    on_query = [fetch(query_hbm.at[pl.ds(k * 512, 512), :], query_w.at[pl.ds(k * 512, 512), :]) for k in range(4)]
    on_key = fetch(key_hbm, key_w)
    on_value = fetch(value_hbm, value_w)
    on_keys, on_values = [], []
    for s in range(4):
        on_keys.append(fetch(cache_keys.at[pl.ds(s * span, span), :], keys.at[pl.ds(s * span, span), :]))
    for s in range(4):
        on_values.append(fetch(cache_values.at[pl.ds(s * span, span), :], values.at[pl.ds(s * span, span), :]))
    on_out = [fetch(out_hbm.at[pl.ds(k * 256, 256), :], out_w.at[pl.ds(k * 256, 256), :]) for k in range(4)]
    ahead = [fetch(gate_hbm, w_gate), fetch(up_hbm, w_up), fetch(down_hbm, w_down)]

    x = tokens[...].astype(f32)
    normed = rms_norm(x, attn_gain[...], 1e-06).astype(bf16)
    query = None
    for k in range(4):
        on_query[k].wait()
        term = dot(normed[:, k * 512 : (k + 1) * 512], query_w[k * 512 : (k + 1) * 512, :])
        query = term if query is None else query + term
    query = query.astype(bf16).astype(f32)
    for s in range(4):
        for h in range(HEADS):
            query_rows[s * 8 + h : s * 8 + h + 1, :] = query[s : s + 1, h * HEAD_DIM : (h + 1) * HEAD_DIM]
    on_key.wait()
    knew = dot(normed, key_w[...]).astype(bf16)
    key_new[...] = knew
    on_value.wait()
    vnew = dot(normed, value_w[...]).astype(bf16)
    value_new[...] = vnew
    knew = knew.astype(f32)
    vnew = vnew.astype(f32)
    first = lax.broadcasted_iota(jnp.int32, (8, HEAD_DIM), 1) < HEAD_DIM // 2
    low_head = lax.broadcasted_iota(jnp.int32, (8, HEAD_DIM), 0) < 4
    lane = lax.broadcasted_iota(jnp.int32, (16, span), 1)
    row = lax.broadcasted_iota(jnp.int32, (16, span), 0)
    own_head = (lane & 1) == ((row >> 2) & 1)
    place = lane >> 1
    scale = (HEAD_DIM // 2) ** (-0.5)
    weights, own_weights = [], []
    for s in range(4):
        q = query_rows[s * 8 : s * 8 + 8, :]
        q = jnp.concatenate([jnp.where(first, q, 0.0), jnp.where(first, 0.0, q)])
        k_own = jnp.where(low_head, knew[s : s + 1, 0:HEAD_DIM], knew[s : s + 1, HEAD_DIM:])
        own = jnp.sum(q * jnp.concatenate([k_own, k_own]), axis=1, keepdims=True) * scale
        on_keys[s].wait()
        scores = dot_last(q.astype(bf16), keys[s * span : (s + 1) * span, :]) * scale
        scores = jnp.where(own_head & (place < lengths[s]), scores, -jnp.inf)
        largest = jnp.maximum(jnp.max(scores, axis=1, keepdims=True), own)
        raised = jnp.exp(scores - largest)
        own_raised = jnp.exp(own - largest)
        total = jnp.sum(raised, axis=1, keepdims=True) + own_raised
        prob = raised / total
        own_prob = own_raised / total
        lam = mix_lambda[...]
        weights.append((prob[0:8] - lam * prob[8:16]).astype(bf16))
        own_weights.append((own_prob[0:8] - lam * own_prob[8:16]).astype(bf16).astype(f32))
    for s in range(4):
        v_own = jnp.where(low_head, vnew[s : s + 1, 0:HEAD_DIM], vnew[s : s + 1, HEAD_DIM:])
        on_values[s].wait()
        mixed = dot(weights[s], values[s * span : (s + 1) * span, :]) + own_weights[s] * v_own
        heads = rms_norm(mixed, head_gain[...], 1e-05)
        for h in range(HEADS):
            head_rows[s : s + 1, h * HEAD_DIM : (h + 1) * HEAD_DIM] = heads[h : h + 1, :]
    heads = head_rows[...].astype(bf16)
    state = x
    for k in range(4):
        on_out[k].wait()
        state = state + dot(heads[:, k * 256 : (k + 1) * 256], out_w[k * 256 : (k + 1) * 256, :])
    hidden[...] = state
    ffn_in = rms_norm(state, ffn_gain[...], 1e-06).astype(bf16)
    lane = lax.broadcasted_iota(jnp.int32, (4, TAIL), 1)
    row = lax.broadcasted_iota(jnp.int32, (4, TAIL), 0)
    tail = jnp.zeros((4, TAIL), f32)
    for t in range(4):
        for k in range(2):
            weight = jnp.full((4, TAIL), route_weights[t, k], f32)
            upper = weight.astype(bf16).astype(f32)
            there = row == t
            tail = jnp.where(there & (lane == routes[t, k]), upper, tail)
            tail = jnp.where(there & (lane == routes[t, k] + 8), weight - upper, tail)
    for half in range(2):
        pair[half, :, 0:HALF] = ffn_in[:, half * HALF : (half + 1) * HALF]
        pair[half, :, HALF:] = tail.astype(bf16)
    for copy in ahead:
        copy.wait()


def pieces_kernel(gate, up, down, out, sem):
    copies = []
    for m, ref in enumerate((gate, up, down)):
        for k in range(8):
            size = min(UNITS, ref.shape[0] - k * UNITS)
            source = ref.at[pl.ds(k * UNITS, size), :]
            target = out.at[k, pl.ds(m * UNITS, size), :]
            copies.append(pltpu.make_async_copy(source, target, sem.at[m * 8 + k]))
            copies[-1].start()
            if size < UNITS:
                out[k, m * UNITS + size : (m + 1) * UNITS, :] = jnp.zeros((UNITS - size, 256), bf16)
    for copy in copies:
        copy.wait()


def dot(a, b):
    return jnp.dot(a, b, preferred_element_type=f32)


def ffn_kernel(ids, own, theirs, pieces, branch, w_gate, w_up, w_down, y_other, y_own, rows, near, far):
    core, expert = ids[0], ids[1]
    for side, ref in enumerate((own, theirs)):
        rows[side] = ref[...].reshape(512, HALF + TAIL)
    near[...] = jnp.zeros_like(near)
    far[...] = jnp.zeros_like(far)
    for b in range(8):
        near[b, 0:UNITS, :] = pieces[b, 0:UNITS, :]
        near[b, 128 : 128 + UNITS, :] = pieces[b, UNITS : 2 * UNITS, :]
        near[b, 64:72, :] = jnp.broadcast_to(branch[:, b * 256 : (b + 1) * 256], (8, 256))
        far[0:UNITS, b * 256 : (b + 1) * 256] = pieces[b, 2 * UNITS :, :]
    halves = (core, 1 - core)
    gate_sum = up_sum = both = None
    for side in range(2):
        base = pl.multiple_of(halves[side] * HALF, HALF)
        x = rows[side, :, 0:HALF]
        gate_part = dot(x, w_gate[pl.ds(base, HALF), :])
        up_part = dot(x, w_up[pl.ds(base, HALF), :])
        gate_sum = gate_part if side == 0 else gate_sum + gate_part
        up_sum = up_part if side == 0 else up_sum + up_part
        for j in range(4):
            xj = rows[side, :, j * 256 : (j + 1) * 256]
            term = lax.dot_general(xj, near[halves[side] * 4 + j], (((1,), (1,)), ((), ())), preferred_element_type=f32)
            both = term if both is None else both + term
    act = (gate_sum * jax.nn.sigmoid(gate_sum) * up_sum).astype(bf16)
    dense_gate = both[:, 0:128]
    dense_act = dense_gate * jax.nn.sigmoid(dense_gate) * both[:, 128:256]
    lane = lax.broadcasted_iota(jnp.int32, (512, 128), 1)
    gate = jax.nn.sigmoid(jnp.sum(jnp.where(lane == 64, dense_gate, 0.0), axis=1, keepdims=True))
    tail = rows[0, :, HALF : HALF + TAIL].astype(f32)
    weight = jnp.sum(jnp.where((lane == expert) | (lane == expert + 8), tail, 0.0), axis=1, keepdims=True)
    dense_act = jnp.where(lane < UNITS, dense_act, 0.0).astype(bf16)
    for side, ref in ((1, y_other), (0, y_own)):
        base = pl.multiple_of(halves[side] * HALF, HALF)
        total = weight * dot(act, w_down[:, pl.ds(base, HALF)]) + gate * dot(dense_act, far[:, pl.ds(base, HALF)])
        ref[...] = total.astype(ref.dtype)


def join_kernel(y_own, y_recv, out):
    out[...] = (y_own[...] + y_recv[...].astype(f32)).astype(bf16).reshape(128, 4, HALF)


def last_kernel(hidden, parts, out):
    for half in range(2):
        total = jnp.zeros((4, HALF), f32)
        for chip in range(64):
            total = total + parts[2 * chip + half].astype(f32)
        cols = slice(half * HALF, (half + 1) * HALF)
        out[:, cols] = (hidden[:, cols] + total).astype(bf16)


def call(kernel, outs, operands, scratch=(), spaces=None):
    spaces = spaces or {}
    operands = [pltpu.with_memory_space_constraint(x, pltpu.HBM) if spaces.get(k) is pltpu.HBM else x for k, x in enumerate(operands)]
    return pl.pallas_call(
        kernel,
        in_specs=[pl.BlockSpec(memory_space=spaces.get(k, pltpu.VMEM)) for k in range(len(operands))],
        out_specs=[pl.BlockSpec(memory_space=pltpu.VMEM)] * len(outs),
        out_shape=[pltpu.VMEM(shape, kind) if local else jax.ShapeDtypeStruct(shape, kind) for shape, kind, local in outs],
        scratch_shapes=list(scratch),
        compiler_params=pltpu.CompilerParams(vmem_limit_bytes=36 * 1024 * 1024),
    )(*operands)


def per_device(
    tokens, lengths, cache_keys, cache_values, query_w, key_w, value_w, out_w, mix_lambda, head_gain, attn_gain, ffn_gain,
    routes, route_weights, exp_gate, exp_up, exp_down, dense_gate, dense_up, dense_down, branch_gate,
):
    rows = tokens.shape[0]
    me = lax.axis_index("ep")
    core = me % 2
    ids = jnp.stack([core, me // 16]).astype(jnp.int32)

    smem, hbm = pltpu.SMEM, pltpu.HBM
    (pieces,) = call(
        pieces_kernel,
        [((8, PIECE, 256), bf16, True)],
        [jnp.swapaxes(dense_gate[0], 0, 1), jnp.swapaxes(dense_up[0], 0, 1), dense_down[0]],
        [pltpu.SemaphoreType.DMA((24,))],
        {0: hbm, 1: hbm, 2: hbm},
    )
    columns = [[16 * b + j for b in range(8)] for j in range(16)]
    pieces = lax.all_to_all(pieces, "ep", 0, 0, axis_index_groups=columns, tiled=True)

    positions = cache_keys.shape[0] * cache_keys.shape[1] * KV_HEADS
    pair, hidden_state, key_new, value_new, w_gate, w_up, w_down = call(
        attend_kernel,
        [
            ((2, rows, HALF + TAIL), bf16, True), ((rows, D), f32, True),
            ((rows, KV_HEADS * HEAD_DIM), bf16, False), ((rows, KV_HEADS * HEAD_DIM), bf16, False),
            (exp_gate.shape, bf16, True), (exp_up.shape, bf16, True), (exp_down.shape, bf16, True),
        ],
        [
            lengths, routes, route_weights, tokens, mix_lambda.reshape(HEADS, 1), head_gain.reshape(1, HEAD_DIM),
            attn_gain.reshape(1, D), ffn_gain.reshape(1, D), query_w, key_w, value_w,
            cache_keys.reshape(positions, HEAD_DIM), cache_values.reshape(positions, HEAD_DIM), out_w, exp_gate, exp_up, exp_down,
        ],
        [
            pltpu.VMEM(query_w.shape, bf16), pltpu.VMEM(key_w.shape, bf16), pltpu.VMEM(value_w.shape, bf16),
            pltpu.VMEM((positions, HEAD_DIM), bf16), pltpu.VMEM((positions, HEAD_DIM), bf16), pltpu.VMEM(out_w.shape, bf16),
            pltpu.SemaphoreType.DMA((21,)), pltpu.VMEM((32, HEAD_DIM), f32), pltpu.VMEM((rows, HEADS * HEAD_DIM), f32),
        ],
        {0: smem, 1: smem, 2: smem, **{k: hbm for k in range(8, 17)}},
    )
    outgoing = jnp.broadcast_to(pair[None], (64, 2, rows, HALF + TAIL)).reshape(DEVICES, rows, HALF + TAIL)
    outgoing, pieces = lax.optimization_barrier((outgoing, pieces))
    own = lax.all_to_all(outgoing, "ep", 0, 0, tiled=True)
    theirs = to_partner(own)
    y_other, y_own = call(
        ffn_kernel,
        [((512, HALF), bf16, True), ((512, HALF), f32, True)],
        [ids, own, theirs, pieces, branch_gate.reshape(1, D), w_gate, w_up, w_down],
        [pltpu.VMEM((2, 512, HALF + TAIL), bf16), pltpu.VMEM((8, 256, 256), bf16), pltpu.VMEM((128, D), bf16)],
        {0: smem},
    )
    y_recv = to_partner(y_other)
    (joined,) = call(join_kernel, [((DEVICES, rows, HALF), bf16, True)], [y_own, y_recv])
    parts = lax.all_to_all(joined, "ep", 0, 0, tiled=True)
    (output,) = call(last_kernel, [((rows, D), bf16, False)], [hidden_state, parts])
    return (output, key_new, value_new)


def solution(mesh):
    placed = (
        P("ep", None),
        P("ep"),
        P("ep", None, None, None),
        P("ep", None, None, None),
        P(),
        P(),
        P(),
        P(),
        P(),
        P(),
        P(),
        P(),
        P("ep", None),
        P("ep", None),
        P(None, "ep"),
        P(None, "ep"),
        P("ep", None),
        P("ep", None, None),
        P("ep", None, None),
        P("ep", None, None),
        P(),
    )

    return jax.shard_map(
        per_device,
        mesh=mesh,
        in_specs=placed,
        out_specs=(P("ep", None), P("ep", None), P("ep", None)),
        check_vma=False,
    )
```

```python
import jax
import jax.numpy as jnp
from jax import lax
from jax.experimental import pallas as pl
from jax.experimental.pallas import tpu as pltpu
from jax.sharding import PartitionSpec as P


HEADS = 8
KV_HEADS = 2
HEAD_DIM = 128
DEVICES = 128
D = 2048
HALF = D // 2
UNITS = 48
PIECE = 3 * UNITS
TAIL = 128
f32 = jnp.float32
bf16 = jnp.bfloat16


def to_partner(x):
    return lax.ppermute(x, "ep", [(i, i ^ 1) for i in range(DEVICES)])


def rms_norm(values, gain, epsilon):
    scale = lax.rsqrt(jnp.mean(values * values, axis=-1, keepdims=True) + epsilon)
    return values * scale * gain


def dot_last(a, b):
    return lax.dot_general(a, b, (((1,), (1,)), ((), ())), preferred_element_type=f32)


def attend_kernel(
    lengths, routes, route_weights, tokens, mix_lambda, head_gain, attn_gain, ffn_gain,
    query_hbm, key_hbm, value_hbm, cache_keys, cache_values, out_hbm,
    pair, hidden, key_new, value_new,
    query_w, key_w, value_w, keys, values, out_w, sem, query_rows, head_rows,
):
    span = keys.shape[0] // 4
    copies = []

    def fetch(source, target):
        copies.append(pltpu.make_async_copy(source, target, sem.at[len(copies)]))
        copies[-1].start()
        return copies[-1]

    on_query = [fetch(query_hbm.at[pl.ds(k * 512, 512), :], query_w.at[pl.ds(k * 512, 512), :]) for k in range(4)]
    on_key = fetch(key_hbm, key_w)
    on_value = fetch(value_hbm, value_w)
    on_keys, on_values = [], []
    for s in range(4):
        on_keys.append(fetch(cache_keys.at[pl.ds(s * span, span), :], keys.at[pl.ds(s * span, span), :]))
    for s in range(4):
        on_values.append(fetch(cache_values.at[pl.ds(s * span, span), :], values.at[pl.ds(s * span, span), :]))
    on_out = [fetch(out_hbm.at[pl.ds(k * 256, 256), :], out_w.at[pl.ds(k * 256, 256), :]) for k in range(4)]

    x = tokens[...].astype(f32)
    normed = rms_norm(x, attn_gain[...], 1e-06).astype(bf16)
    query = None
    for k in range(4):
        on_query[k].wait()
        term = dot(normed[:, k * 512 : (k + 1) * 512], query_w[k * 512 : (k + 1) * 512, :])
        query = term if query is None else query + term
    query = query.astype(bf16).astype(f32)
    for s in range(4):
        for h in range(HEADS):
            query_rows[s * 8 + h : s * 8 + h + 1, :] = query[s : s + 1, h * HEAD_DIM : (h + 1) * HEAD_DIM]
    on_key.wait()
    knew = dot(normed, key_w[...]).astype(bf16)
    key_new[...] = knew
    on_value.wait()
    vnew = dot(normed, value_w[...]).astype(bf16)
    value_new[...] = vnew
    knew = knew.astype(f32)
    vnew = vnew.astype(f32)
    first = lax.broadcasted_iota(jnp.int32, (8, HEAD_DIM), 1) < HEAD_DIM // 2
    low_head = lax.broadcasted_iota(jnp.int32, (8, HEAD_DIM), 0) < 4
    lane = lax.broadcasted_iota(jnp.int32, (16, span), 1)
    row = lax.broadcasted_iota(jnp.int32, (16, span), 0)
    own_head = (lane & 1) == ((row >> 2) & 1)
    place = lane >> 1
    scale = (HEAD_DIM // 2) ** (-0.5)
    weights, own_weights = [], []
    for s in range(4):
        q = query_rows[s * 8 : s * 8 + 8, :]
        q = jnp.concatenate([jnp.where(first, q, 0.0), jnp.where(first, 0.0, q)])
        k_own = jnp.where(low_head, knew[s : s + 1, 0:HEAD_DIM], knew[s : s + 1, HEAD_DIM:])
        own = jnp.sum(q * jnp.concatenate([k_own, k_own]), axis=1, keepdims=True) * scale
        on_keys[s].wait()
        scores = dot_last(q.astype(bf16), keys[s * span : (s + 1) * span, :]) * scale
        scores = jnp.where(own_head & (place < lengths[s]), scores, -jnp.inf)
        largest = jnp.maximum(jnp.max(scores, axis=1, keepdims=True), own)
        raised = jnp.exp(scores - largest)
        own_raised = jnp.exp(own - largest)
        total = jnp.sum(raised, axis=1, keepdims=True) + own_raised
        prob = raised / total
        own_prob = own_raised / total
        lam = mix_lambda[...]
        weights.append((prob[0:8] - lam * prob[8:16]).astype(bf16))
        own_weights.append((own_prob[0:8] - lam * own_prob[8:16]).astype(bf16).astype(f32))
    for s in range(4):
        v_own = jnp.where(low_head, vnew[s : s + 1, 0:HEAD_DIM], vnew[s : s + 1, HEAD_DIM:])
        on_values[s].wait()
        mixed = dot(weights[s], values[s * span : (s + 1) * span, :]) + own_weights[s] * v_own
        heads = rms_norm(mixed, head_gain[...], 1e-05)
        for h in range(HEADS):
            head_rows[s : s + 1, h * HEAD_DIM : (h + 1) * HEAD_DIM] = heads[h : h + 1, :]
    heads = head_rows[...].astype(bf16)
    state = x
    for k in range(4):
        on_out[k].wait()
        state = state + dot(heads[:, k * 256 : (k + 1) * 256], out_w[k * 256 : (k + 1) * 256, :])
    hidden[...] = state
    ffn_in = rms_norm(state, ffn_gain[...], 1e-06).astype(bf16)
    lane = lax.broadcasted_iota(jnp.int32, (4, TAIL), 1)
    row = lax.broadcasted_iota(jnp.int32, (4, TAIL), 0)
    tail = jnp.zeros((4, TAIL), f32)
    for t in range(4):
        for k in range(2):
            weight = jnp.full((4, TAIL), route_weights[t, k], f32)
            upper = weight.astype(bf16).astype(f32)
            there = row == t
            tail = jnp.where(there & (lane == routes[t, k]), upper, tail)
            tail = jnp.where(there & (lane == routes[t, k] + 8), weight - upper, tail)
    for half in range(2):
        pair[half, :, 0:HALF] = ffn_in[:, half * HALF : (half + 1) * HALF]
        pair[half, :, HALF:] = tail.astype(bf16)


def pieces_kernel(gate, up, down, out, held, sem):
    copies = [pltpu.make_async_copy(ref, held.at[m], sem.at[m]) for m, ref in enumerate((gate, up, down))]
    for copy in copies:
        copy.start()
    for m in range(3):
        copies[m].wait()
        for k in range(8):
            size = min(UNITS, held.shape[1] - k * UNITS)
            out[k, m * UNITS : m * UNITS + size, :] = held[m, k * UNITS : k * UNITS + size, :]
            if size < UNITS:
                out[k, m * UNITS + size : (m + 1) * UNITS, :] = jnp.zeros((UNITS - size, 256), bf16)


def dot(a, b):
    return jnp.dot(a, b, preferred_element_type=f32)


def half_sums(x, w_gate, w_up, near, first):
    both = None
    for j in range(4):
        term = dot_last(x[:, j * 256 : (j + 1) * 256], near[first + j])
        both = term if both is None else both + term
    return dot(x, w_gate), dot(x, w_up), both


def near_kernel(
    ids, own, pieces, branch, gate_hbm, up_hbm, down_hbm,
    gate_sum, up_sum, both, near, far, gate_rest, up_rest, w_down,
    w_gate, w_up, sem,
):
    core = ids[0]
    mine = pl.ds(pl.multiple_of(core * HALF, HALF), HALF)
    rest = pl.ds(pl.multiple_of((1 - core) * HALF, HALF), HALF)
    copies = [
        pltpu.make_async_copy(source, target, sem.at[k])
        for k, (source, target) in enumerate(
            (
                (gate_hbm.at[mine, :], w_gate), (up_hbm.at[mine, :], w_up),
                (gate_hbm.at[rest, :], gate_rest), (up_hbm.at[rest, :], up_rest), (down_hbm, w_down),
            )
        )
    ]
    for copy in copies:
        copy.start()
    near[...] = jnp.zeros_like(near)
    far[...] = jnp.zeros_like(far)
    for b in range(8):
        near[b, 0:UNITS, :] = pieces[b, 0:UNITS, :]
        near[b, 128 : 128 + UNITS, :] = pieces[b, UNITS : 2 * UNITS, :]
        near[b, 64:72, :] = jnp.broadcast_to(branch[:, b * 256 : (b + 1) * 256], (8, 256))
        far[0:UNITS, b * 256 : (b + 1) * 256] = pieces[b, 2 * UNITS :, :]
    x = own[:, :, 0:HALF].reshape(512, HALF)
    copies[0].wait()
    copies[1].wait()
    gate_sum[...], up_sum[...], both[...] = half_sums(x, w_gate[...], w_up[...], near, core * 4)
    for copy in copies[2:]:
        copy.wait()


def out_half(act, dense_act, weight, gate, w_down, far, half):
    columns = pl.ds(pl.multiple_of(half * HALF, HALF), HALF)
    return weight * dot(act, w_down[:, columns]) + gate * dot(dense_act, far[:, columns])


def rest_kernel(
    ids, theirs, gate_near, up_near, both_near, near, far, gate_rest, up_rest, w_down, y_other, act_out, dense_out, scales
):
    core, expert = ids[0], ids[1]
    x = theirs[:, :, 0:HALF].reshape(512, HALF)
    gate_sum, up_sum, both = half_sums(x, gate_rest[...], up_rest[...], near, (1 - core) * 4)
    gate_sum = gate_sum + gate_near[...]
    up_sum = up_sum + up_near[...]
    both = both + both_near[...]
    act = (gate_sum * jax.nn.sigmoid(gate_sum) * up_sum).astype(bf16)
    dense_gate = both[:, 0:128]
    dense_act = dense_gate * jax.nn.sigmoid(dense_gate) * both[:, 128:256]
    lane = lax.broadcasted_iota(jnp.int32, (512, 128), 1)
    gate = jax.nn.sigmoid(jnp.sum(jnp.where(lane == 64, dense_gate, 0.0), axis=1, keepdims=True))
    tail = theirs[:, :, HALF : HALF + TAIL].reshape(512, TAIL).astype(f32)
    weight = jnp.sum(jnp.where((lane == expert) | (lane == expert + 8), tail, 0.0), axis=1, keepdims=True)
    dense_act = jnp.where(lane < UNITS, dense_act, 0.0).astype(bf16)
    act_out[...] = act
    dense_out[...] = dense_act
    scales[0] = jnp.broadcast_to(weight, (512, 128))
    scales[1] = jnp.broadcast_to(gate, (512, 128))
    y_other[...] = out_half(act, dense_act, weight, gate, w_down, far, 1 - core).astype(bf16)


def own_kernel(ids, act, dense_act, scales, far, w_down, y_own):
    y_own[...] = out_half(act[...], dense_act[...], scales[0, :, 0:1], scales[1, :, 0:1], w_down, far, ids[0])


def join_kernel(y_own, y_recv, out):
    out[...] = (y_own[...] + y_recv[...].astype(f32)).astype(bf16).reshape(128, 4, HALF)


def last_kernel(hidden, parts, out):
    for half in range(2):
        total = jnp.zeros((4, HALF), f32)
        for chip in range(64):
            total = total + parts[2 * chip + half].astype(f32)
        cols = slice(half * HALF, (half + 1) * HALF)
        out[:, cols] = (hidden[:, cols] + total).astype(bf16)


def call(kernel, outs, operands, scratch=(), spaces=None):
    spaces = spaces or {}
    operands = [pltpu.with_memory_space_constraint(x, pltpu.HBM) if spaces.get(k) is pltpu.HBM else x for k, x in enumerate(operands)]
    return pl.pallas_call(
        kernel,
        in_specs=[pl.BlockSpec(memory_space=spaces.get(k, pltpu.VMEM)) for k in range(len(operands))],
        out_specs=[pl.BlockSpec(memory_space=pltpu.VMEM)] * len(outs),
        out_shape=[pltpu.VMEM(shape, kind) if local else jax.ShapeDtypeStruct(shape, kind) for shape, kind, local in outs],
        scratch_shapes=list(scratch),
        compiler_params=pltpu.CompilerParams(vmem_limit_bytes=36 * 1024 * 1024),
    )(*operands)


def per_device(
    tokens, lengths, cache_keys, cache_values, query_w, key_w, value_w, out_w, mix_lambda, head_gain, attn_gain, ffn_gain,
    routes, route_weights, exp_gate, exp_up, exp_down, dense_gate, dense_up, dense_down, branch_gate,
):
    rows = tokens.shape[0]
    me = lax.axis_index("ep")
    core = me % 2
    ids = jnp.stack([core, me // 16]).astype(jnp.int32)

    smem, hbm = pltpu.SMEM, pltpu.HBM
    (pieces,) = call(
        pieces_kernel,
        [((8, PIECE, 256), bf16, True)],
        [jnp.swapaxes(dense_gate[0], 0, 1), jnp.swapaxes(dense_up[0], 0, 1), dense_down[0]],
        [pltpu.VMEM((3, 352, 256), bf16), pltpu.SemaphoreType.DMA((3,))],
        {0: hbm, 1: hbm, 2: hbm},
    )
    columns = [[16 * b + j for b in range(8)] for j in range(16)]
    pieces = lax.all_to_all(pieces, "ep", 0, 0, axis_index_groups=columns, tiled=True)

    positions = cache_keys.shape[0] * cache_keys.shape[1] * KV_HEADS
    pair, hidden_state, key_new, value_new = call(
        attend_kernel,
        [
            ((2, rows, HALF + TAIL), bf16, True), ((rows, D), f32, True),
            ((rows, KV_HEADS * HEAD_DIM), bf16, False), ((rows, KV_HEADS * HEAD_DIM), bf16, False),
        ],
        [
            lengths, routes, route_weights, tokens, mix_lambda.reshape(HEADS, 1), head_gain.reshape(1, HEAD_DIM),
            attn_gain.reshape(1, D), ffn_gain.reshape(1, D), query_w, key_w, value_w,
            cache_keys.reshape(positions, HEAD_DIM), cache_values.reshape(positions, HEAD_DIM), out_w,
        ],
        [
            pltpu.VMEM(query_w.shape, bf16), pltpu.VMEM(key_w.shape, bf16), pltpu.VMEM(value_w.shape, bf16),
            pltpu.VMEM((positions, HEAD_DIM), bf16), pltpu.VMEM((positions, HEAD_DIM), bf16), pltpu.VMEM(out_w.shape, bf16),
            pltpu.SemaphoreType.DMA((18,)), pltpu.VMEM((32, HEAD_DIM), f32), pltpu.VMEM((rows, HEADS * HEAD_DIM), f32),
        ],
        {0: smem, 1: smem, 2: smem, **{k: hbm for k in range(8, 14)}},
    )
    outgoing = jnp.broadcast_to(pair[None], (64, 2, rows, HALF + TAIL)).reshape(DEVICES, rows, HALF + TAIL)
    outgoing, pieces = lax.optimization_barrier((outgoing, pieces))
    own = lax.all_to_all(outgoing, "ep", 0, 0, tiled=True)
    theirs = to_partner(own)
    hidden_units = exp_gate.shape[1]
    gate_near, up_near, both_near, near, far, gate_rest, up_rest, w_down = call(
        near_kernel,
        [
            ((512, hidden_units), f32, True), ((512, hidden_units), f32, True), ((512, 256), f32, True),
            ((8, 256, 256), bf16, True), ((128, D), bf16, True),
            ((HALF, hidden_units), bf16, True), ((HALF, hidden_units), bf16, True), (exp_down.shape, bf16, True),
        ],
        [ids, own, pieces, branch_gate.reshape(1, D), exp_gate, exp_up, exp_down],
        [pltpu.VMEM((HALF, hidden_units), bf16), pltpu.VMEM((HALF, hidden_units), bf16), pltpu.SemaphoreType.DMA((5,))],
        {0: smem, 4: hbm, 5: hbm, 6: hbm},
    )
    y_other, act, dense_act, scales = call(
        rest_kernel,
        [((512, HALF), bf16, True), ((512, hidden_units), bf16, True), ((512, 128), bf16, True), ((2, 512, 128), f32, True)],
        [ids, theirs, gate_near, up_near, both_near, near, far, gate_rest, up_rest, w_down],
        [],
        {0: smem},
    )
    y_recv = to_partner(y_other)
    (y_own,) = call(own_kernel, [((512, HALF), f32, True)], [ids, act, dense_act, scales, far, w_down], [], {0: smem})
    (joined,) = call(join_kernel, [((DEVICES, rows, HALF), bf16, True)], [y_own, y_recv])
    parts = lax.all_to_all(joined, "ep", 0, 0, tiled=True)
    (output,) = call(last_kernel, [((rows, D), bf16, False)], [hidden_state, parts])
    return (output, key_new, value_new)


def solution(mesh):
    placed = (
        P("ep", None),
        P("ep"),
        P("ep", None, None, None),
        P("ep", None, None, None),
        P(),
        P(),
        P(),
        P(),
        P(),
        P(),
        P(),
        P(),
        P("ep", None),
        P("ep", None),
        P(None, "ep"),
        P(None, "ep"),
        P("ep", None),
        P("ep", None, None),
        P("ep", None, None),
        P("ep", None, None),
        P(),
    )

    return jax.shard_map(
        per_device,
        mesh=mesh,
        in_specs=placed,
        out_specs=(P("ep", None), P("ep", None), P("ep", None)),
        check_vma=False,
    )
```

```python
import jax
import jax.numpy as jnp
from jax import lax
from jax.experimental import pallas as pl
from jax.experimental.pallas import tpu as pltpu
from jax.sharding import PartitionSpec as P


HEADS = 8
KV_HEADS = 2
HEAD_DIM = 128
DEVICES = 128
D = 2048
HALF = D // 2
UNITS = 48
PIECE = 3 * UNITS
TAIL = 128
f32 = jnp.float32
bf16 = jnp.bfloat16


def to_partner(x):
    return lax.ppermute(x, "ep", [(i, i ^ 1) for i in range(DEVICES)])


def rms_norm(values, gain, epsilon):
    scale = lax.rsqrt(jnp.mean(values * values, axis=-1, keepdims=True) + epsilon)
    return values * scale * gain


def dot_last(a, b):
    return lax.dot_general(a, b, (((1,), (1,)), ((), ())), preferred_element_type=f32)


def attend_kernel(
    lengths_hbm, routes_hbm, route_weights_hbm, tokens_hbm, mix_hbm, head_gain_hbm, attn_gain_hbm, ffn_gain_hbm,
    query_hbm, key_hbm, value_hbm, cache_keys, cache_values, out_hbm,
    pair, hidden, key_out, value_out,
    query_w, key_w, value_w, keys, values, out_w, sem, query_rows, head_rows,
    lengths, routes, route_weights, tokens, mix_lambda, head_gain, attn_gain, ffn_gain, key_new, value_new,
):
    span = keys.shape[0] // 4
    copies = []

    def fetch(source, target):
        copies.append(pltpu.make_async_copy(source, target, sem.at[len(copies)]))
        copies[-1].start()
        return copies[-1]

    on_tokens = [fetch(tokens_hbm, tokens), fetch(attn_gain_hbm, attn_gain)]
    on_query = [fetch(query_hbm.at[pl.ds(k * 512, 512), :], query_w.at[pl.ds(k * 512, 512), :]) for k in range(4)]
    on_key = fetch(key_hbm, key_w)
    on_value = fetch(value_hbm, value_w)
    on_small = [
        fetch(lengths_hbm, lengths), fetch(mix_hbm, mix_lambda), fetch(head_gain_hbm, head_gain), fetch(ffn_gain_hbm, ffn_gain),
        fetch(routes_hbm, routes), fetch(route_weights_hbm, route_weights),
    ]
    on_keys, on_values = [], []
    for s in range(4):
        on_keys.append(fetch(cache_keys.at[pl.ds(s * span, span), :], keys.at[pl.ds(s * span, span), :]))
    for s in range(4):
        on_values.append(fetch(cache_values.at[pl.ds(s * span, span), :], values.at[pl.ds(s * span, span), :]))
    on_out = [fetch(out_hbm.at[pl.ds(k * 256, 256), :], out_w.at[pl.ds(k * 256, 256), :]) for k in range(4)]

    for copy in on_tokens:
        copy.wait()
    x = tokens[...].astype(f32)
    normed = rms_norm(x, attn_gain[...], 1e-06).astype(bf16)
    query = None
    for k in range(4):
        on_query[k].wait()
        term = dot(normed[:, k * 512 : (k + 1) * 512], query_w[k * 512 : (k + 1) * 512, :])
        query = term if query is None else query + term
    query = query.astype(bf16).astype(f32)
    for s in range(4):
        for h in range(HEADS):
            query_rows[s * 8 + h : s * 8 + h + 1, :] = query[s : s + 1, h * HEAD_DIM : (h + 1) * HEAD_DIM]
    for copy in on_small:
        copy.wait()
    lane = lax.broadcasted_iota(jnp.int32, (4, TAIL), 1)
    row = lax.broadcasted_iota(jnp.int32, (4, TAIL), 0)
    tail = jnp.zeros((4, TAIL), f32)
    for t in range(4):
        for k in range(2):
            weight = jnp.full((4, TAIL), route_weights[k, t], f32)
            upper = weight.astype(bf16).astype(f32)
            there = row == t
            tail = jnp.where(there & (lane == routes[k, t]), upper, tail)
            tail = jnp.where(there & (lane == routes[k, t] + 8), weight - upper, tail)
    for half in range(2):
        pair[half, :, HALF:] = tail.astype(bf16)
    on_key.wait()
    knew = dot(normed, key_w[...]).astype(bf16)
    key_new[...] = knew
    written = [fetch(key_new, key_out)]
    on_value.wait()
    vnew = dot(normed, value_w[...]).astype(bf16)
    value_new[...] = vnew
    written.append(fetch(value_new, value_out))
    knew = knew.astype(f32)
    vnew = vnew.astype(f32)
    first = lax.broadcasted_iota(jnp.int32, (8, HEAD_DIM), 1) < HEAD_DIM // 2
    low_head = lax.broadcasted_iota(jnp.int32, (8, HEAD_DIM), 0) < 4
    lane = lax.broadcasted_iota(jnp.int32, (16, span), 1)
    row = lax.broadcasted_iota(jnp.int32, (16, span), 0)
    own_head = (lane & 1) == ((row >> 2) & 1)
    place = lane >> 1
    scale = (HEAD_DIM // 2) ** (-0.5)
    weights, own_weights = [], []
    lam = jnp.zeros((8, 1), f32)
    head = lax.broadcasted_iota(jnp.int32, (8, 1), 0)
    for h in range(HEADS):
        lam = jnp.where(head == h, mix_lambda[h], lam)
    for s in range(4):
        q = query_rows[s * 8 : s * 8 + 8, :]
        q = jnp.concatenate([jnp.where(first, q, 0.0), jnp.where(first, 0.0, q)])
        k_own = jnp.where(low_head, knew[s : s + 1, 0:HEAD_DIM], knew[s : s + 1, HEAD_DIM:])
        own = jnp.sum(q * jnp.concatenate([k_own, k_own]), axis=1, keepdims=True) * scale
        on_keys[s].wait()
        scores = dot_last(q.astype(bf16), keys[s * span : (s + 1) * span, :]) * scale
        scores = jnp.where(own_head & (place < lengths[s]), scores, -jnp.inf)
        largest = jnp.maximum(jnp.max(scores, axis=1, keepdims=True), own)
        raised = jnp.exp(scores - largest)
        own_raised = jnp.exp(own - largest)
        total = jnp.sum(raised, axis=1, keepdims=True) + own_raised
        prob = raised / total
        own_prob = own_raised / total
        weights.append((prob[0:8] - lam * prob[8:16]).astype(bf16))
        own_weights.append((own_prob[0:8] - lam * own_prob[8:16]).astype(bf16).astype(f32))
    for s in range(4):
        v_own = jnp.where(low_head, vnew[s : s + 1, 0:HEAD_DIM], vnew[s : s + 1, HEAD_DIM:])
        on_values[s].wait()
        mixed = dot(weights[s], values[s * span : (s + 1) * span, :]) + own_weights[s] * v_own
        heads = rms_norm(mixed, head_gain[...], 1e-05)
        for h in range(HEADS):
            head_rows[s : s + 1, h * HEAD_DIM : (h + 1) * HEAD_DIM] = heads[h : h + 1, :]
    heads = head_rows[...].astype(bf16)
    state = x
    for k in range(4):
        on_out[k].wait()
        state = state + dot(heads[:, k * 256 : (k + 1) * 256], out_w[k * 256 : (k + 1) * 256, :])
    hidden[...] = state
    ffn_in = rms_norm(state, ffn_gain[...], 1e-06).astype(bf16)
    for half in range(2):
        pair[half, :, 0:HALF] = ffn_in[:, half * HALF : (half + 1) * HALF]
    for copy in written:
        copy.wait()


def pieces_kernel(gate, up, down, out, held, sem):
    copies = [pltpu.make_async_copy(ref, held.at[m], sem.at[m]) for m, ref in enumerate((gate, up, down))]
    for copy in copies:
        copy.start()
    for m in range(3):
        copies[m].wait()
        for k in range(8):
            size = min(UNITS, held.shape[1] - k * UNITS)
            out[k, m * UNITS : m * UNITS + size, :] = held[m, k * UNITS : k * UNITS + size, :]
            if size < UNITS:
                out[k, m * UNITS + size : (m + 1) * UNITS, :] = jnp.zeros((UNITS - size, 256), bf16)


def dot(a, b):
    return jnp.dot(a, b, preferred_element_type=f32)


def dense_sums(x, near, first):
    both = None
    for j in range(4):
        term = dot_last(x[:, j * 256 : (j + 1) * 256], near[first + j])
        both = term if both is None else both + term
    return both


def near_kernel(ids, own, pieces, branch, gate_hbm, up_hbm, down_hbm, sums, both, near, w_rest, w_out, w_own, sem):
    core = ids[0]
    mine = pl.ds(pl.multiple_of(core * HALF, HALF), HALF)
    rest = pl.ds(pl.multiple_of((1 - core) * HALF, HALF), HALF)
    wide = gate_hbm.shape[1]
    left, right = pl.ds(0, wide), pl.ds(wide, wide)
    copies = [
        pltpu.make_async_copy(source, target, sem.at[k])
        for k, (source, target) in enumerate(
            (
                (gate_hbm.at[mine, :], w_own.at[:, left]), (up_hbm.at[mine, :], w_own.at[:, right]),
                (gate_hbm.at[rest, :], w_rest.at[:, left]), (up_hbm.at[rest, :], w_rest.at[:, right]),
                (down_hbm, w_out.at[pl.ds(0, wide), :]),
            )
        )
    ]
    for copy in copies:
        copy.start()
    near[...] = jnp.zeros_like(near)
    w_out[wide + UNITS :, :] = jnp.zeros((128 - UNITS, D), bf16)
    for b in range(8):
        near[b, 0:UNITS, :] = pieces[b, 0:UNITS, :]
        near[b, 128 : 128 + UNITS, :] = pieces[b, UNITS : 2 * UNITS, :]
        near[b, 64:72, :] = jnp.broadcast_to(branch[:, b * 256 : (b + 1) * 256], (8, 256))
        w_out[wide : wide + UNITS, b * 256 : (b + 1) * 256] = pieces[b, 2 * UNITS :, :]
    x = own[:, :, 0:HALF].reshape(512, HALF)
    both[...] = dense_sums(x, near, core * 4)
    copies[0].wait()
    copies[1].wait()
    sums[...] = dot(x, w_own[...])
    for copy in copies[2:]:
        copy.wait()


def rest_kernel(ids, theirs, sums_near, both_near, near, w_rest, w_out, y_other, acts):
    core, expert = ids[0], ids[1]
    x = theirs[:, :, 0:HALF].reshape(512, HALF)
    both = dense_sums(x, near, (1 - core) * 4) + both_near[...]
    sums = dot(x, w_rest[...]) + sums_near[...]
    wide = sums.shape[1] // 2
    gate_sum, up_sum = sums[:, 0:wide], sums[:, wide:]
    dense_gate = both[:, 0:128]
    lane = lax.broadcasted_iota(jnp.int32, (512, 128), 1)
    gate = jax.nn.sigmoid(jnp.sum(jnp.where(lane == 64, dense_gate, 0.0), axis=1, keepdims=True))
    tail = theirs[:, :, HALF : HALF + TAIL].reshape(512, TAIL).astype(f32)
    weight = jnp.sum(jnp.where((lane == expert) | (lane == expert + 8), tail, 0.0), axis=1, keepdims=True)
    dense_act = gate * (dense_gate * jax.nn.sigmoid(dense_gate) * both[:, 128:256])
    acts[:, 0:wide] = (weight * (gate_sum * jax.nn.sigmoid(gate_sum) * up_sum)).astype(bf16)
    acts[:, wide:] = jnp.where(lane < UNITS, dense_act, 0.0).astype(bf16)
    columns = pl.ds(pl.multiple_of((1 - core) * HALF, HALF), HALF)
    y_other[...] = dot(acts[...], w_out[:, columns]).astype(bf16)


def own_kernel(ids, acts, w_out, y_own):
    y_own[...] = dot(acts[...], w_out[:, pl.ds(pl.multiple_of(ids[0] * HALF, HALF), HALF)])


def join_kernel(y_own, y_recv, out):
    out[...] = (y_own[...] + y_recv[...].astype(f32)).astype(bf16).reshape(128, 4, HALF)


def last_kernel(hidden, parts, out):
    for half in range(2):
        total = jnp.zeros((4, HALF), f32)
        for chip in range(64):
            total = total + parts[2 * chip + half].astype(f32)
        cols = slice(half * HALF, (half + 1) * HALF)
        out[:, cols] = (hidden[:, cols] + total).astype(bf16)


def call(kernel, outs, operands, scratch=(), spaces=None):
    spaces = spaces or {}
    operands = [pltpu.with_memory_space_constraint(x, pltpu.HBM) if spaces.get(k) is pltpu.HBM else x for k, x in enumerate(operands)]
    return pl.pallas_call(
        kernel,
        in_specs=[pl.BlockSpec(memory_space=spaces.get(k, pltpu.VMEM)) for k in range(len(operands))],
        out_specs=[pl.BlockSpec(memory_space=space or pltpu.VMEM) for _, _, space in outs],
        out_shape=[space(shape, kind) if space else jax.ShapeDtypeStruct(shape, kind) for shape, kind, space in outs],
        scratch_shapes=list(scratch),
        compiler_params=pltpu.CompilerParams(vmem_limit_bytes=36 * 1024 * 1024),
    )(*operands)


def per_device(
    tokens, lengths, cache_keys, cache_values, query_w, key_w, value_w, out_w, mix_lambda, head_gain, attn_gain, ffn_gain,
    routes, route_weights, exp_gate, exp_up, exp_down, dense_gate, dense_up, dense_down, branch_gate,
):
    rows = tokens.shape[0]
    me = lax.axis_index("ep")
    core = me % 2
    ids = jnp.stack([core, me // 16]).astype(jnp.int32)

    smem, hbm, vmem = pltpu.SMEM, pltpu.HBM, pltpu.VMEM
    (pieces,) = call(
        pieces_kernel,
        [((8, PIECE, 256), bf16, vmem)],
        [jnp.swapaxes(dense_gate[0], 0, 1), jnp.swapaxes(dense_up[0], 0, 1), dense_down[0]],
        [pltpu.VMEM((3, 352, 256), bf16), pltpu.SemaphoreType.DMA((3,))],
        {0: hbm, 1: hbm, 2: hbm},
    )
    columns = [[16 * b + j for b in range(8)] for j in range(16)]
    pieces = lax.all_to_all(pieces, "ep", 0, 0, axis_index_groups=columns, tiled=True)

    positions = cache_keys.shape[0] * cache_keys.shape[1] * KV_HEADS
    pair, hidden_state, key_new, value_new = call(
        attend_kernel,
        [
            ((2, rows, HALF + TAIL), bf16, vmem), ((rows, D), f32, vmem),
            ((rows, KV_HEADS * HEAD_DIM), bf16, hbm), ((rows, KV_HEADS * HEAD_DIM), bf16, hbm),
        ],
        [
            lengths, routes.T, route_weights.T, tokens, mix_lambda, head_gain.reshape(1, HEAD_DIM),
            attn_gain.reshape(1, D), ffn_gain.reshape(1, D), query_w, key_w, value_w,
            cache_keys.reshape(positions, HEAD_DIM), cache_values.reshape(positions, HEAD_DIM), out_w,
        ],
        [
            pltpu.VMEM(query_w.shape, bf16), pltpu.VMEM(key_w.shape, bf16), pltpu.VMEM(value_w.shape, bf16),
            pltpu.VMEM((positions, HEAD_DIM), bf16), pltpu.VMEM((positions, HEAD_DIM), bf16), pltpu.VMEM(out_w.shape, bf16),
            pltpu.SemaphoreType.DMA((28,)), pltpu.VMEM((32, HEAD_DIM), f32), pltpu.VMEM((rows, HEADS * HEAD_DIM), f32),
            pltpu.SMEM((rows,), jnp.int32), pltpu.SMEM((2, rows), jnp.int32), pltpu.SMEM((2, rows), f32), pltpu.VMEM((rows, D), bf16),
            pltpu.SMEM((HEADS,), f32), pltpu.VMEM((1, HEAD_DIM), f32), pltpu.VMEM((1, D), f32), pltpu.VMEM((1, D), f32),
            pltpu.VMEM((rows, KV_HEADS * HEAD_DIM), bf16), pltpu.VMEM((rows, KV_HEADS * HEAD_DIM), bf16),
        ],
        {k: hbm for k in range(14)},
    )
    outgoing = jnp.broadcast_to(pair[None], (64, 2, rows, HALF + TAIL)).reshape(DEVICES, rows, HALF + TAIL)
    outgoing, pieces = lax.optimization_barrier((outgoing, pieces))
    own = lax.all_to_all(outgoing, "ep", 0, 0, tiled=True)
    theirs = to_partner(own)
    hidden_units = exp_gate.shape[1]
    sums, both, near, w_rest, w_out = call(
        near_kernel,
        [
            ((512, 2 * hidden_units), f32, vmem), ((512, 256), f32, vmem), ((8, 256, 256), bf16, vmem),
            ((HALF, 2 * hidden_units), bf16, vmem), ((hidden_units + 128, D), bf16, vmem),
        ],
        [ids, own, pieces, branch_gate.reshape(1, D), exp_gate, exp_up, exp_down],
        [pltpu.VMEM((HALF, 2 * hidden_units), bf16), pltpu.SemaphoreType.DMA((5,))],
        {0: smem, 4: hbm, 5: hbm, 6: hbm},
    )
    y_other, acts = call(
        rest_kernel,
        [((512, HALF), bf16, vmem), ((512, hidden_units + 128), bf16, vmem)],
        [ids, theirs, sums, both, near, w_rest, w_out],
        [],
        {0: smem},
    )
    y_recv = to_partner(y_other)
    (y_own,) = call(own_kernel, [((512, HALF), f32, vmem)], [ids, acts, w_out], [], {0: smem})
    (joined,) = call(join_kernel, [((DEVICES, rows, HALF), bf16, vmem)], [y_own, y_recv])
    parts = lax.all_to_all(joined, "ep", 0, 0, tiled=True)
    (output,) = call(last_kernel, [((rows, D), bf16, None)], [hidden_state, parts])
    return (output, key_new, value_new)


def solution(mesh):
    placed = (
        P("ep", None),
        P("ep"),
        P("ep", None, None, None),
        P("ep", None, None, None),
        P(),
        P(),
        P(),
        P(),
        P(),
        P(),
        P(),
        P(),
        P("ep", None),
        P("ep", None),
        P(None, "ep"),
        P(None, "ep"),
        P("ep", None),
        P("ep", None, None),
        P("ep", None, None),
        P("ep", None, None),
        P(),
    )

    return jax.shard_map(
        per_device,
        mesh=mesh,
        in_specs=placed,
        out_specs=(P("ep", None), P("ep", None), P("ep", None)),
        check_vma=False,
    )
```

```python
import jax
import jax.numpy as jnp
from jax import lax
from jax.experimental import pallas as pl
from jax.experimental.pallas import tpu as pltpu
from jax.sharding import PartitionSpec as P


HEADS = 8
KV_HEADS = 2
HEAD_DIM = 128
DEVICES = 128
D = 2048
HALF = D // 2
UNITS = 48
PIECE = 3 * UNITS
TAIL = 128
f32 = jnp.float32
bf16 = jnp.bfloat16


def to_partner(x):
    return lax.ppermute(x, "ep", [(i, i ^ 1) for i in range(DEVICES)])


def rms_norm(values, gain, epsilon):
    scale = lax.rsqrt(jnp.mean(values * values, axis=-1, keepdims=True) + epsilon)
    return values * scale * gain


def dot_last(a, b):
    return lax.dot_general(a, b, (((1,), (1,)), ((), ())), preferred_element_type=f32)


def attend_kernel(
    lengths_hbm, routes_hbm, route_weights_hbm, tokens_hbm, mix_hbm, head_gain_hbm, attn_gain_hbm, ffn_gain_hbm,
    query_hbm, key_hbm, value_hbm, cache_keys, cache_values, out_hbm,
    pair, hidden, key_out, value_out,
    query_w, key_w, value_w, keys, values, out_w, sem, query_rows, head_rows,
    lengths, routes, route_weights, tokens, mix_lambda, head_gain, attn_gain, ffn_gain, key_new, value_new,
):
    span = keys.shape[0] // 4
    copies = []

    def fetch(source, target):
        copies.append(pltpu.make_async_copy(source, target, sem.at[len(copies)]))
        copies[-1].start()
        return copies[-1]

    on_tokens = [fetch(tokens_hbm, tokens), fetch(attn_gain_hbm, attn_gain)]
    on_query = [fetch(query_hbm.at[pl.ds(k * 512, 512), :], query_w.at[pl.ds(k * 512, 512), :]) for k in range(4)]
    on_key = fetch(key_hbm, key_w)
    on_value = fetch(value_hbm, value_w)
    on_small = [
        fetch(lengths_hbm, lengths), fetch(mix_hbm, mix_lambda), fetch(head_gain_hbm, head_gain), fetch(ffn_gain_hbm, ffn_gain),
        fetch(routes_hbm, routes), fetch(route_weights_hbm, route_weights),
    ]
    on_keys, on_values = [], []
    for s in range(4):
        on_keys.append(fetch(cache_keys.at[pl.ds(s * span, span), :], keys.at[pl.ds(s * span, span), :]))
    for s in range(4):
        on_values.append(fetch(cache_values.at[pl.ds(s * span, span), :], values.at[pl.ds(s * span, span), :]))
    on_out = [fetch(out_hbm.at[pl.ds(k * 256, 256), :], out_w.at[pl.ds(k * 256, 256), :]) for k in range(4)]

    for copy in on_tokens:
        copy.wait()
    x = tokens[...].astype(f32)
    normed = rms_norm(x, attn_gain[...], 1e-06).astype(bf16)
    query = None
    for k in range(4):
        on_query[k].wait()
        term = dot(normed[:, k * 512 : (k + 1) * 512], query_w[k * 512 : (k + 1) * 512, :])
        query = term if query is None else query + term
    query = query.astype(bf16).astype(f32)
    for s in range(4):
        for h in range(HEADS):
            query_rows[s * 8 + h : s * 8 + h + 1, :] = query[s : s + 1, h * HEAD_DIM : (h + 1) * HEAD_DIM]
    for copy in on_small:
        copy.wait()
    lane = lax.broadcasted_iota(jnp.int32, (4, TAIL), 1)
    row = lax.broadcasted_iota(jnp.int32, (4, TAIL), 0)
    tail = jnp.zeros((4, TAIL), f32)
    for t in range(4):
        for k in range(2):
            weight = jnp.full((4, TAIL), route_weights[k, t], f32)
            upper = weight.astype(bf16).astype(f32)
            there = row == t
            tail = jnp.where(there & (lane == routes[k, t]), upper, tail)
            tail = jnp.where(there & (lane == routes[k, t] + 8), weight - upper, tail)
    for half in range(2):
        pair[half, :, HALF:] = tail.astype(bf16)
    on_key.wait()
    knew = dot(normed, key_w[...]).astype(bf16)
    key_new[...] = knew
    written = [fetch(key_new, key_out)]
    on_value.wait()
    vnew = dot(normed, value_w[...]).astype(bf16)
    value_new[...] = vnew
    written.append(fetch(value_new, value_out))
    knew = knew.astype(f32)
    vnew = vnew.astype(f32)
    first = lax.broadcasted_iota(jnp.int32, (8, HEAD_DIM), 1) < HEAD_DIM // 2
    low_head = lax.broadcasted_iota(jnp.int32, (8, HEAD_DIM), 0) < 4
    lane = lax.broadcasted_iota(jnp.int32, (16, span), 1)
    row = lax.broadcasted_iota(jnp.int32, (16, span), 0)
    own_head = (lane & 1) == ((row >> 2) & 1)
    place = lane >> 1
    scale = (HEAD_DIM // 2) ** (-0.5)
    weights, own_weights = [], []
    lam = jnp.zeros((8, 1), f32)
    head = lax.broadcasted_iota(jnp.int32, (8, 1), 0)
    for h in range(HEADS):
        lam = jnp.where(head == h, mix_lambda[h], lam)
    for s in range(4):
        q = query_rows[s * 8 : s * 8 + 8, :]
        q = jnp.concatenate([jnp.where(first, q, 0.0), jnp.where(first, 0.0, q)])
        k_own = jnp.where(low_head, knew[s : s + 1, 0:HEAD_DIM], knew[s : s + 1, HEAD_DIM:])
        own = jnp.sum(q * jnp.concatenate([k_own, k_own]), axis=1, keepdims=True) * scale
        on_keys[s].wait()
        scores = dot_last(q.astype(bf16), keys[s * span : (s + 1) * span, :]) * scale
        scores = jnp.where(own_head & (place < lengths[s]), scores, -jnp.inf)
        largest = jnp.maximum(jnp.max(scores, axis=1, keepdims=True), own)
        raised = jnp.exp(scores - largest)
        own_raised = jnp.exp(own - largest)
        total = jnp.sum(raised, axis=1, keepdims=True) + own_raised
        prob = raised / total
        own_prob = own_raised / total
        weights.append((prob[0:8] - lam * prob[8:16]).astype(bf16))
        own_weights.append((own_prob[0:8] - lam * own_prob[8:16]).astype(bf16).astype(f32))
    for s in range(4):
        v_own = jnp.where(low_head, vnew[s : s + 1, 0:HEAD_DIM], vnew[s : s + 1, HEAD_DIM:])
        on_values[s].wait()
        mixed = dot(weights[s], values[s * span : (s + 1) * span, :]) + own_weights[s] * v_own
        heads = rms_norm(mixed, head_gain[...], 1e-05)
        for h in range(HEADS):
            head_rows[s : s + 1, h * HEAD_DIM : (h + 1) * HEAD_DIM] = heads[h : h + 1, :]
    heads = head_rows[...].astype(bf16)
    state = x
    for k in range(4):
        on_out[k].wait()
        state = state + dot(heads[:, k * 256 : (k + 1) * 256], out_w[k * 256 : (k + 1) * 256, :])
    hidden[...] = state
    ffn_in = rms_norm(state, ffn_gain[...], 1e-06).astype(bf16)
    for half in range(2):
        pair[half, :, 0:HALF] = ffn_in[:, half * HALF : (half + 1) * HALF]
    for copy in written:
        copy.wait()


def pieces_kernel(ids, gate, up, down, *refs):
    outs, held, sem = refs[:4], refs[4], refs[5]
    copies = [
        pltpu.make_async_copy(ref, held.at[m, pl.ds(0, ref.shape[0]), :], sem.at[m]) for m, ref in enumerate((gate, up, down))
    ]
    for copy in copies:
        copy.start()
    held[:, gate.shape[0] :, :] = jnp.zeros((3, 8 * UNITS - gate.shape[0], 256), bf16)
    for m in range(3):
        copies[m].wait()
        for k in range(4):
            for side in range(2):
                run = 2 * jnp.bitwise_and(ids[3] + k, 3) + jnp.bitwise_xor(ids[2], side)
                start = pl.multiple_of(run * UNITS, 16)
                at = side * PIECE + m * UNITS
                outs[k][at : at + UNITS, :] = held[m, pl.ds(start, UNITS), :]


def dot(a, b):
    return jnp.dot(a, b, preferred_element_type=f32)


def dense_sums(x, near, first):
    both = None
    for j in range(4):
        term = dot_last(x[:, j * 256 : (j + 1) * 256], near[first + j])
        both = term if both is None else both + term
    return both


def near_kernel(ids, own, first, second, third, fourth, crossed, branch, gate_hbm, up_hbm, down_hbm, sums, both, near, w_rest, w_out, w_own, sem):
    core = ids[0]
    mine = pl.ds(pl.multiple_of(core * HALF, HALF), HALF)
    rest = pl.ds(pl.multiple_of((1 - core) * HALF, HALF), HALF)
    wide = gate_hbm.shape[1]
    left, right = pl.ds(0, wide), pl.ds(wide, wide)
    copies = [
        pltpu.make_async_copy(source, target, sem.at[k])
        for k, (source, target) in enumerate(
            (
                (gate_hbm.at[mine, :], w_own.at[:, left]), (up_hbm.at[mine, :], w_own.at[:, right]),
                (gate_hbm.at[rest, :], w_rest.at[:, left]), (up_hbm.at[rest, :], w_rest.at[:, right]),
                (down_hbm, w_out.at[pl.ds(0, wide), :]),
            )
        )
    ]
    for copy in copies:
        copy.start()
    near[...] = jnp.zeros_like(near)
    w_out[wide + UNITS :, :] = jnp.zeros((128 - UNITS, D), bf16)
    for b in range(8):
        near[b, 64:72, :] = jnp.broadcast_to(branch[:, b * 256 : (b + 1) * 256], (8, 256))
    for k, ref in enumerate((first, second, third, fourth)):
        for side in range(2):
            block = 2 * jnp.bitwise_and(ids[3] + 4 - k, 3) + jnp.bitwise_xor(ids[2], side)
            piece = ref[0:PIECE, :] if side == 0 else crossed[k]
            near[block, 0:UNITS, :] = piece[0:UNITS, :]
            near[block, 128 : 128 + UNITS, :] = piece[UNITS : 2 * UNITS, :]
            w_out[wide : wide + UNITS, pl.ds(pl.multiple_of(block * 256, 256), 256)] = piece[2 * UNITS :, :]
    x = own[:, :, 0:HALF].reshape(512, HALF)
    both[...] = dense_sums(x, near, core * 4)
    copies[0].wait()
    copies[1].wait()
    sums[...] = dot(x, w_own[...])
    for copy in copies[2:]:
        copy.wait()


def rest_kernel(ids, theirs, sums_near, both_near, near, w_rest, w_out, y_other, acts):
    core, expert = ids[0], ids[1]
    x = theirs[:, :, 0:HALF].reshape(512, HALF)
    both = dense_sums(x, near, (1 - core) * 4) + both_near[...]
    sums = dot(x, w_rest[...]) + sums_near[...]
    wide = sums.shape[1] // 2
    gate_sum, up_sum = sums[:, 0:wide], sums[:, wide:]
    dense_gate = both[:, 0:128]
    lane = lax.broadcasted_iota(jnp.int32, (512, 128), 1)
    gate = jax.nn.sigmoid(jnp.sum(jnp.where(lane == 64, dense_gate, 0.0), axis=1, keepdims=True))
    tail = theirs[:, :, HALF : HALF + TAIL].reshape(512, TAIL).astype(f32)
    weight = jnp.sum(jnp.where((lane == expert) | (lane == expert + 8), tail, 0.0), axis=1, keepdims=True)
    dense_act = gate * (dense_gate * jax.nn.sigmoid(dense_gate) * both[:, 128:256])
    acts[:, 0:wide] = (weight * (gate_sum * jax.nn.sigmoid(gate_sum) * up_sum)).astype(bf16)
    acts[:, wide:] = jnp.where(lane < UNITS, dense_act, 0.0).astype(bf16)
    columns = pl.ds(pl.multiple_of((1 - core) * HALF, HALF), HALF)
    y_other[...] = dot(acts[...], w_out[:, columns]).astype(bf16)


def own_kernel(ids, acts, w_out, y_own):
    y_own[...] = dot(acts[...], w_out[:, pl.ds(pl.multiple_of(ids[0] * HALF, HALF), HALF)])


def join_kernel(y_own, y_recv, out):
    out[...] = (y_own[...] + y_recv[...].astype(f32)).astype(bf16).reshape(128, 4, HALF)


def last_kernel(hidden, parts, out):
    for half in range(2):
        total = jnp.zeros((4, HALF), f32)
        for chip in range(64):
            total = total + parts[2 * chip + half].astype(f32)
        cols = slice(half * HALF, (half + 1) * HALF)
        out[:, cols] = (hidden[:, cols] + total).astype(bf16)


def call(kernel, outs, operands, scratch=(), spaces=None):
    spaces = spaces or {}
    operands = [pltpu.with_memory_space_constraint(x, pltpu.HBM) if spaces.get(k) is pltpu.HBM else x for k, x in enumerate(operands)]
    return pl.pallas_call(
        kernel,
        in_specs=[pl.BlockSpec(memory_space=spaces.get(k, pltpu.VMEM)) for k in range(len(operands))],
        out_specs=[pl.BlockSpec(memory_space=space or pltpu.VMEM) for _, _, space in outs],
        out_shape=[space(shape, kind) if space else jax.ShapeDtypeStruct(shape, kind) for shape, kind, space in outs],
        scratch_shapes=list(scratch),
        compiler_params=pltpu.CompilerParams(vmem_limit_bytes=36 * 1024 * 1024),
    )(*operands)


def per_device(
    tokens, lengths, cache_keys, cache_values, query_w, key_w, value_w, out_w, mix_lambda, head_gain, attn_gain, ffn_gain,
    routes, route_weights, exp_gate, exp_up, exp_down, dense_gate, dense_up, dense_down, branch_gate,
):
    rows = tokens.shape[0]
    me = lax.axis_index("ep")
    core = me % 2
    ids = jnp.stack([core, me // 16, me // 16 % 2, me // 32]).astype(jnp.int32)

    smem, hbm, vmem = pltpu.SMEM, pltpu.HBM, pltpu.VMEM
    pieces = call(
        pieces_kernel,
        [((2 * PIECE, 256), bf16, vmem)] * 4,
        [ids, jnp.swapaxes(dense_gate[0], 0, 1), jnp.swapaxes(dense_up[0], 0, 1), dense_down[0]],
        [pltpu.VMEM((3, 8 * UNITS, 256), bf16), pltpu.SemaphoreType.DMA((3,))],
        {0: smem, 1: hbm, 2: hbm, 3: hbm},
    )
    turned = [lax.ppermute(pieces[k], "ep", [(i, (i + 32 * k) % DEVICES) for i in range(DEVICES)]) for k in (1, 3, 2)]
    pieces = [pieces[0], turned[0], turned[2], turned[1]]

    positions = cache_keys.shape[0] * cache_keys.shape[1] * KV_HEADS
    pair, hidden_state, key_new, value_new = call(
        attend_kernel,
        [
            ((2, rows, HALF + TAIL), bf16, vmem), ((rows, D), f32, vmem),
            ((rows, KV_HEADS * HEAD_DIM), bf16, hbm), ((rows, KV_HEADS * HEAD_DIM), bf16, hbm),
        ],
        [
            lengths, routes.T, route_weights.T, tokens, mix_lambda, head_gain.reshape(1, HEAD_DIM),
            attn_gain.reshape(1, D), ffn_gain.reshape(1, D), query_w, key_w, value_w,
            cache_keys.reshape(positions, HEAD_DIM), cache_values.reshape(positions, HEAD_DIM), out_w,
        ],
        [
            pltpu.VMEM(query_w.shape, bf16), pltpu.VMEM(key_w.shape, bf16), pltpu.VMEM(value_w.shape, bf16),
            pltpu.VMEM((positions, HEAD_DIM), bf16), pltpu.VMEM((positions, HEAD_DIM), bf16), pltpu.VMEM(out_w.shape, bf16),
            pltpu.SemaphoreType.DMA((28,)), pltpu.VMEM((32, HEAD_DIM), f32), pltpu.VMEM((rows, HEADS * HEAD_DIM), f32),
            pltpu.SMEM((rows,), jnp.int32), pltpu.SMEM((2, rows), jnp.int32), pltpu.SMEM((2, rows), f32), pltpu.VMEM((rows, D), bf16),
            pltpu.SMEM((HEADS,), f32), pltpu.VMEM((1, HEAD_DIM), f32), pltpu.VMEM((1, D), f32), pltpu.VMEM((1, D), f32),
            pltpu.VMEM((rows, KV_HEADS * HEAD_DIM), bf16), pltpu.VMEM((rows, KV_HEADS * HEAD_DIM), bf16),
        ],
        {k: hbm for k in range(14)},
    )
    outgoing = jnp.broadcast_to(pair[None], (64, 2, rows, HALF + TAIL)).reshape(DEVICES, rows, HALF + TAIL)
    crossed = lax.ppermute(jnp.stack([x[PIECE:] for x in pieces]), "ep", [(i, i ^ 16) for i in range(DEVICES)])
    own = lax.all_to_all(outgoing, "ep", 0, 0, tiled=True)
    theirs = to_partner(own)
    hidden_units = exp_gate.shape[1]
    sums, both, near, w_rest, w_out = call(
        near_kernel,
        [
            ((512, 2 * hidden_units), f32, vmem), ((512, 256), f32, vmem), ((8, 256, 256), bf16, vmem),
            ((HALF, 2 * hidden_units), bf16, vmem), ((hidden_units + 128, D), bf16, vmem),
        ],
        [ids, own, *pieces, crossed, branch_gate.reshape(1, D), exp_gate, exp_up, exp_down],
        [pltpu.VMEM((HALF, 2 * hidden_units), bf16), pltpu.SemaphoreType.DMA((5,))],
        {0: smem, 8: hbm, 9: hbm, 10: hbm},
    )
    y_other, acts = call(
        rest_kernel,
        [((512, HALF), bf16, vmem), ((512, hidden_units + 128), bf16, vmem)],
        [ids, theirs, sums, both, near, w_rest, w_out],
        [],
        {0: smem},
    )
    y_recv = to_partner(y_other)
    (y_own,) = call(own_kernel, [((512, HALF), f32, vmem)], [ids, acts, w_out], [], {0: smem})
    (joined,) = call(join_kernel, [((DEVICES, rows, HALF), bf16, vmem)], [y_own, y_recv])
    parts = lax.all_to_all(joined, "ep", 0, 0, tiled=True)
    (output,) = call(last_kernel, [((rows, D), bf16, None)], [hidden_state, parts])
    return (output, key_new, value_new)


def solution(mesh):
    placed = (
        P("ep", None),
        P("ep"),
        P("ep", None, None, None),
        P("ep", None, None, None),
        P(),
        P(),
        P(),
        P(),
        P(),
        P(),
        P(),
        P(),
        P("ep", None),
        P("ep", None),
        P(None, "ep"),
        P(None, "ep"),
        P("ep", None),
        P("ep", None, None),
        P("ep", None, None),
        P("ep", None, None),
        P(),
    )

    return jax.shard_map(
        per_device,
        mesh=mesh,
        in_specs=placed,
        out_specs=(P("ep", None), P("ep", None), P("ep", None)),
        check_vma=False,
    )
```

```python
import jax
import jax.numpy as jnp
from jax import lax
from jax.experimental import pallas as pl
from jax.experimental.pallas import tpu as pltpu
from jax.sharding import PartitionSpec as P


HEADS = 8
KV_HEADS = 2
HEAD_DIM = 128
DEVICES = 128
D = 2048
HALF = D // 2
UNITS = 48
PIECE = 3 * UNITS
TAIL = 128
f32 = jnp.float32
bf16 = jnp.bfloat16


def to_partner(x):
    return lax.ppermute(x, "ep", [(i, i ^ 1) for i in range(DEVICES)])


def rms_norm(values, gain, epsilon):
    scale = lax.rsqrt(jnp.mean(values * values, axis=-1, keepdims=True) + epsilon)
    return values * scale * gain


def dot_last(a, b):
    return lax.dot_general(a, b, (((1,), (1,)), ((), ())), preferred_element_type=f32)


def attend_kernel(
    ids, lengths_hbm, routes_hbm, route_weights_hbm, tokens_hbm, mix_hbm, head_gain_hbm, attn_gain_hbm, ffn_gain_hbm,
    query_hbm, key_hbm, value_hbm, cache_keys, cache_values, out_hbm,
    gate_hbm, up_hbm, down_hbm,
    pair, hidden, key_out, value_out, w_own, w_rest, w_down,
    query_w, key_w, value_w, keys, values, out_w, sem, query_rows, head_rows,
    lengths, routes, route_weights, tokens, mix_lambda, head_gain, attn_gain, ffn_gain, key_new, value_new,
):
    span = keys.shape[0] // 4
    copies = []

    def fetch(source, target):
        copies.append(pltpu.make_async_copy(source, target, sem.at[len(copies)]))
        copies[-1].start()
        return copies[-1]

    on_tokens = [fetch(tokens_hbm, tokens), fetch(attn_gain_hbm, attn_gain)]
    on_query = [fetch(query_hbm.at[pl.ds(k * 512, 512), :], query_w.at[pl.ds(k * 512, 512), :]) for k in range(4)]
    on_key = fetch(key_hbm, key_w)
    on_value = fetch(value_hbm, value_w)
    on_small = [
        fetch(lengths_hbm, lengths), fetch(mix_hbm, mix_lambda), fetch(head_gain_hbm, head_gain), fetch(ffn_gain_hbm, ffn_gain),
        fetch(routes_hbm, routes), fetch(route_weights_hbm, route_weights),
    ]
    on_keys, on_values = [], []
    for s in range(4):
        on_keys.append(fetch(cache_keys.at[pl.ds(s * span, span), :], keys.at[pl.ds(s * span, span), :]))
    for s in range(4):
        on_values.append(fetch(cache_values.at[pl.ds(s * span, span), :], values.at[pl.ds(s * span, span), :]))
    on_out = [fetch(out_hbm.at[pl.ds(k * 256, 256), :], out_w.at[pl.ds(k * 256, 256), :]) for k in range(4)]

    wide = gate_hbm.shape[1]
    ahead = [fetch(down_hbm, w_down)]
    for half, target in ((ids[0], w_own), (1 - ids[0], w_rest)):
        rows = pl.ds(pl.multiple_of(half * HALF, HALF), HALF)
        ahead.append(fetch(gate_hbm.at[rows, :], target.at[:, pl.ds(0, wide)]))
        ahead.append(fetch(up_hbm.at[rows, :], target.at[:, pl.ds(wide, wide)]))
    for copy in on_tokens:
        copy.wait()
    x = tokens[...].astype(f32)
    normed = rms_norm(x, attn_gain[...], 1e-06).astype(bf16)
    query = None
    for k in range(4):
        on_query[k].wait()
        term = dot(normed[:, k * 512 : (k + 1) * 512], query_w[k * 512 : (k + 1) * 512, :])
        query = term if query is None else query + term
    query = query.astype(bf16).astype(f32)
    for s in range(4):
        for h in range(HEADS):
            query_rows[s * 8 + h : s * 8 + h + 1, :] = query[s : s + 1, h * HEAD_DIM : (h + 1) * HEAD_DIM]
    for copy in on_small:
        copy.wait()
    lane = lax.broadcasted_iota(jnp.int32, (4, TAIL), 1)
    row = lax.broadcasted_iota(jnp.int32, (4, TAIL), 0)
    tail = jnp.zeros((4, TAIL), f32)
    for t in range(4):
        for k in range(2):
            weight = jnp.full((4, TAIL), route_weights[k, t], f32)
            upper = weight.astype(bf16).astype(f32)
            there = row == t
            tail = jnp.where(there & (lane == routes[k, t]), upper, tail)
            tail = jnp.where(there & (lane == routes[k, t] + 8), weight - upper, tail)
    for half in range(2):
        pair[half, :, HALF:] = tail.astype(bf16)
    on_key.wait()
    knew = dot(normed, key_w[...]).astype(bf16)
    key_new[...] = knew
    written = [fetch(key_new, key_out)]
    on_value.wait()
    vnew = dot(normed, value_w[...]).astype(bf16)
    value_new[...] = vnew
    written.append(fetch(value_new, value_out))
    knew = knew.astype(f32)
    vnew = vnew.astype(f32)
    first = lax.broadcasted_iota(jnp.int32, (8, HEAD_DIM), 1) < HEAD_DIM // 2
    low_head = lax.broadcasted_iota(jnp.int32, (8, HEAD_DIM), 0) < 4
    lane = lax.broadcasted_iota(jnp.int32, (16, span), 1)
    row = lax.broadcasted_iota(jnp.int32, (16, span), 0)
    own_head = (lane & 1) == ((row >> 2) & 1)
    place = lane >> 1
    scale = (HEAD_DIM // 2) ** (-0.5)
    weights, own_weights = [], []
    lam = jnp.zeros((8, 1), f32)
    head = lax.broadcasted_iota(jnp.int32, (8, 1), 0)
    for h in range(HEADS):
        lam = jnp.where(head == h, mix_lambda[h], lam)
    for s in range(4):
        q = query_rows[s * 8 : s * 8 + 8, :]
        q = jnp.concatenate([jnp.where(first, q, 0.0), jnp.where(first, 0.0, q)])
        k_own = jnp.where(low_head, knew[s : s + 1, 0:HEAD_DIM], knew[s : s + 1, HEAD_DIM:])
        own = jnp.sum(q * jnp.concatenate([k_own, k_own]), axis=1, keepdims=True) * scale
        on_keys[s].wait()
        scores = dot_last(q.astype(bf16), keys[s * span : (s + 1) * span, :]) * scale
        scores = jnp.where(own_head & (place < lengths[s]), scores, -jnp.inf)
        largest = jnp.maximum(jnp.max(scores, axis=1, keepdims=True), own)
        raised = jnp.exp(scores - largest)
        own_raised = jnp.exp(own - largest)
        total = jnp.sum(raised, axis=1, keepdims=True) + own_raised
        prob = raised / total
        own_prob = own_raised / total
        weights.append((prob[0:8] - lam * prob[8:16]).astype(bf16))
        own_weights.append((own_prob[0:8] - lam * own_prob[8:16]).astype(bf16).astype(f32))
    for s in range(4):
        v_own = jnp.where(low_head, vnew[s : s + 1, 0:HEAD_DIM], vnew[s : s + 1, HEAD_DIM:])
        on_values[s].wait()
        mixed = dot(weights[s], values[s * span : (s + 1) * span, :]) + own_weights[s] * v_own
        heads = rms_norm(mixed, head_gain[...], 1e-05)
        for h in range(HEADS):
            head_rows[s : s + 1, h * HEAD_DIM : (h + 1) * HEAD_DIM] = heads[h : h + 1, :]
    heads = head_rows[...].astype(bf16)
    state = x
    for k in range(4):
        on_out[k].wait()
        state = state + dot(heads[:, k * 256 : (k + 1) * 256], out_w[k * 256 : (k + 1) * 256, :])
    hidden[...] = state
    ffn_in = rms_norm(state, ffn_gain[...], 1e-06).astype(bf16)
    for half in range(2):
        pair[half, :, 0:HALF] = ffn_in[:, half * HALF : (half + 1) * HALF]
    for copy in written + ahead:
        copy.wait()


def pieces_kernel(ids, gate, up, down, *refs):
    outs, held, sem = refs[:4], refs[4], refs[5]
    copies = [
        pltpu.make_async_copy(ref, held.at[m, pl.ds(0, ref.shape[0]), :], sem.at[m]) for m, ref in enumerate((gate, up, down))
    ]
    for copy in copies:
        copy.start()
    held[:, gate.shape[0] :, :] = jnp.zeros((3, 8 * UNITS - gate.shape[0], 256), bf16)
    for m in range(3):
        copies[m].wait()
        for k in range(4):
            for side in range(2):
                run = 2 * jnp.bitwise_and(ids[3] + k, 3) + jnp.bitwise_xor(ids[2], side)
                start = pl.multiple_of(run * UNITS, 16)
                at = side * PIECE + m * UNITS
                outs[k][at : at + UNITS, :] = held[m, pl.ds(start, UNITS), :]


def dot(a, b):
    return jnp.dot(a, b, preferred_element_type=f32)


def dense_sums(x, near, first):
    both = None
    for j in range(4):
        term = dot_last(x[:, j * 256 : (j + 1) * 256], near[first + j])
        both = term if both is None else both + term
    return both


def near_kernel(ids, own, first, second, third, fourth, crossed, branch, w_own, w_down, sums, both, near, w_out, sem):
    core = ids[0]
    wide = w_down.shape[0]
    copy = pltpu.make_async_copy(w_down, w_out.at[pl.ds(0, wide), :], sem)
    copy.start()
    near[...] = jnp.zeros_like(near)
    w_out[wide + UNITS :, :] = jnp.zeros((128 - UNITS, D), bf16)
    for b in range(8):
        near[b, 64:72, :] = jnp.broadcast_to(branch[:, b * 256 : (b + 1) * 256], (8, 256))
    for k, ref in enumerate((first, second, third, fourth)):
        for side in range(2):
            block = 2 * jnp.bitwise_and(ids[3] + 4 - k, 3) + jnp.bitwise_xor(ids[2], side)
            piece = ref[0:PIECE, :] if side == 0 else crossed[k]
            near[block, 0:UNITS, :] = piece[0:UNITS, :]
            near[block, 128 : 128 + UNITS, :] = piece[UNITS : 2 * UNITS, :]
            w_out[wide : wide + UNITS, pl.ds(pl.multiple_of(block * 256, 256), 256)] = piece[2 * UNITS :, :]
    x = own[:, :, 0:HALF].reshape(512, HALF)
    both[...] = dense_sums(x, near, core * 4)
    sums[...] = dot(x, w_own[...])
    copy.wait()


def rest_kernel(ids, theirs, sums_near, both_near, near, w_rest, w_out, y_other, acts):
    core, expert = ids[0], ids[1]
    x = theirs[:, :, 0:HALF].reshape(512, HALF)
    both = dense_sums(x, near, (1 - core) * 4) + both_near[...]
    sums = dot(x, w_rest[...]) + sums_near[...]
    wide = sums.shape[1] // 2
    gate_sum, up_sum = sums[:, 0:wide], sums[:, wide:]
    dense_gate = both[:, 0:128]
    lane = lax.broadcasted_iota(jnp.int32, (512, 128), 1)
    gate = jax.nn.sigmoid(jnp.sum(jnp.where(lane == 64, dense_gate, 0.0), axis=1, keepdims=True))
    tail = theirs[:, :, HALF : HALF + TAIL].reshape(512, TAIL).astype(f32)
    weight = jnp.sum(jnp.where((lane == expert) | (lane == expert + 8), tail, 0.0), axis=1, keepdims=True)
    dense_act = gate * (dense_gate * jax.nn.sigmoid(dense_gate) * both[:, 128:256])
    acts[:, 0:wide] = (weight * (gate_sum * jax.nn.sigmoid(gate_sum) * up_sum)).astype(bf16)
    acts[:, wide:] = jnp.where(lane < UNITS, dense_act, 0.0).astype(bf16)
    columns = pl.ds(pl.multiple_of((1 - core) * HALF, HALF), HALF)
    y_other[...] = dot(acts[...], w_out[:, columns]).astype(bf16)


def own_kernel(ids, acts, w_out, y_own):
    y_own[...] = dot(acts[...], w_out[:, pl.ds(pl.multiple_of(ids[0] * HALF, HALF), HALF)])


def join_kernel(y_own, y_recv, out):
    out[...] = (y_own[...] + y_recv[...].astype(f32)).astype(bf16).reshape(128, 4, HALF)


def last_kernel(hidden, parts, out):
    for half in range(2):
        total = jnp.zeros((4, HALF), f32)
        for chip in range(64):
            total = total + parts[2 * chip + half].astype(f32)
        cols = slice(half * HALF, (half + 1) * HALF)
        out[:, cols] = (hidden[:, cols] + total).astype(bf16)


def call(kernel, outs, operands, scratch=(), spaces=None):
    spaces = spaces or {}
    operands = [pltpu.with_memory_space_constraint(x, pltpu.HBM) if spaces.get(k) is pltpu.HBM else x for k, x in enumerate(operands)]
    return pl.pallas_call(
        kernel,
        in_specs=[pl.BlockSpec(memory_space=spaces.get(k, pltpu.VMEM)) for k in range(len(operands))],
        out_specs=[pl.BlockSpec(memory_space=space or pltpu.VMEM) for _, _, space in outs],
        out_shape=[space(shape, kind) if space else jax.ShapeDtypeStruct(shape, kind) for shape, kind, space in outs],
        scratch_shapes=list(scratch),
        compiler_params=pltpu.CompilerParams(vmem_limit_bytes=36 * 1024 * 1024),
    )(*operands)


def per_device(
    tokens, lengths, cache_keys, cache_values, query_w, key_w, value_w, out_w, mix_lambda, head_gain, attn_gain, ffn_gain,
    routes, route_weights, exp_gate, exp_up, exp_down, dense_gate, dense_up, dense_down, branch_gate,
):
    rows = tokens.shape[0]
    hidden_units = exp_gate.shape[1]
    me = lax.axis_index("ep")
    core = me % 2
    ids = jnp.stack([core, me // 16, me // 16 % 2, me // 32]).astype(jnp.int32)

    smem, hbm, vmem = pltpu.SMEM, pltpu.HBM, pltpu.VMEM
    pieces = call(
        pieces_kernel,
        [((2 * PIECE, 256), bf16, vmem)] * 4,
        [ids, jnp.swapaxes(dense_gate[0], 0, 1), jnp.swapaxes(dense_up[0], 0, 1), dense_down[0]],
        [pltpu.VMEM((3, 8 * UNITS, 256), bf16), pltpu.SemaphoreType.DMA((3,))],
        {0: smem, 1: hbm, 2: hbm, 3: hbm},
    )
    turned = [lax.ppermute(pieces[k], "ep", [(i, (i + 32 * k) % DEVICES) for i in range(DEVICES)]) for k in (1, 3, 2)]
    pieces = [pieces[0], turned[0], turned[2], turned[1]]

    positions = cache_keys.shape[0] * cache_keys.shape[1] * KV_HEADS
    pair, hidden_state, key_new, value_new, w_own, w_rest, w_down = call(
        attend_kernel,
        [
            ((2, rows, HALF + TAIL), bf16, vmem), ((rows, D), f32, vmem),
            ((rows, KV_HEADS * HEAD_DIM), bf16, hbm), ((rows, KV_HEADS * HEAD_DIM), bf16, hbm),
            ((HALF, 2 * hidden_units), bf16, vmem), ((HALF, 2 * hidden_units), bf16, vmem), (exp_down.shape, bf16, vmem),
        ],
        [
            ids, lengths, routes.T, route_weights.T, tokens, mix_lambda, head_gain.reshape(1, HEAD_DIM),
            attn_gain.reshape(1, D), ffn_gain.reshape(1, D), query_w, key_w, value_w,
            cache_keys.reshape(positions, HEAD_DIM), cache_values.reshape(positions, HEAD_DIM), out_w, exp_gate, exp_up, exp_down,
        ],
        [
            pltpu.VMEM(query_w.shape, bf16), pltpu.VMEM(key_w.shape, bf16), pltpu.VMEM(value_w.shape, bf16),
            pltpu.VMEM((positions, HEAD_DIM), bf16), pltpu.VMEM((positions, HEAD_DIM), bf16), pltpu.VMEM(out_w.shape, bf16),
            pltpu.SemaphoreType.DMA((33,)), pltpu.VMEM((32, HEAD_DIM), f32), pltpu.VMEM((rows, HEADS * HEAD_DIM), f32),
            pltpu.SMEM((rows,), jnp.int32), pltpu.SMEM((2, rows), jnp.int32), pltpu.SMEM((2, rows), f32), pltpu.VMEM((rows, D), bf16),
            pltpu.SMEM((HEADS,), f32), pltpu.VMEM((1, HEAD_DIM), f32), pltpu.VMEM((1, D), f32), pltpu.VMEM((1, D), f32),
            pltpu.VMEM((rows, KV_HEADS * HEAD_DIM), bf16), pltpu.VMEM((rows, KV_HEADS * HEAD_DIM), bf16),
        ],
        {0: smem, **{k: hbm for k in range(1, 18)}},
    )
    outgoing = jnp.broadcast_to(pair[None], (64, 2, rows, HALF + TAIL)).reshape(DEVICES, rows, HALF + TAIL)
    crossed = lax.ppermute(jnp.stack([x[PIECE:] for x in pieces]), "ep", [(i, i ^ 16) for i in range(DEVICES)])
    own = lax.all_to_all(outgoing, "ep", 0, 0, tiled=True)
    theirs = to_partner(own)
    sums, both, near, w_out = call(
        near_kernel,
        [
            ((512, 2 * hidden_units), f32, vmem), ((512, 256), f32, vmem), ((8, 256, 256), bf16, vmem),
            ((hidden_units + 128, D), bf16, vmem),
        ],
        [ids, own, *pieces, crossed, branch_gate.reshape(1, D), w_own, w_down],
        [pltpu.SemaphoreType.DMA],
        {0: smem},
    )
    y_other, acts = call(
        rest_kernel,
        [((512, HALF), bf16, vmem), ((512, hidden_units + 128), bf16, vmem)],
        [ids, theirs, sums, both, near, w_rest, w_out],
        [],
        {0: smem},
    )
    y_recv = to_partner(y_other)
    (y_own,) = call(own_kernel, [((512, HALF), f32, vmem)], [ids, acts, w_out], [], {0: smem})
    (joined,) = call(join_kernel, [((DEVICES, rows, HALF), bf16, vmem)], [y_own, y_recv])
    parts = lax.all_to_all(joined, "ep", 0, 0, tiled=True)
    (output,) = call(last_kernel, [((rows, D), bf16, None)], [hidden_state, parts])
    return (output, key_new, value_new)


def solution(mesh):
    placed = (
        P("ep", None),
        P("ep"),
        P("ep", None, None, None),
        P("ep", None, None, None),
        P(),
        P(),
        P(),
        P(),
        P(),
        P(),
        P(),
        P(),
        P("ep", None),
        P("ep", None),
        P(None, "ep"),
        P(None, "ep"),
        P("ep", None),
        P("ep", None, None),
        P("ep", None, None),
        P("ep", None, None),
        P(),
    )

    return jax.shard_map(
        per_device,
        mesh=mesh,
        in_specs=placed,
        out_specs=(P("ep", None), P("ep", None), P("ep", None)),
        check_vma=False,
    )
```

```python
import jax
import jax.numpy as jnp
from jax import lax
from jax.experimental import pallas as pl
from jax.experimental.pallas import tpu as pltpu
from jax.sharding import PartitionSpec as P


HEADS = 8
KV_HEADS = 2
HEAD_DIM = 128
DEVICES = 128
D = 2048
HALF = D // 2
UNITS = 48
PIECE = 3 * UNITS
TAIL = 128
f32 = jnp.float32
bf16 = jnp.bfloat16


def to_partner(x):
    return lax.ppermute(x, "ep", [(i, i ^ 1) for i in range(DEVICES)])


def rms_norm(values, gain, epsilon):
    scale = lax.rsqrt(jnp.mean(values * values, axis=-1, keepdims=True) + epsilon)
    return values * scale * gain


def dot_last(a, b):
    return lax.dot_general(a, b, (((1,), (1,)), ((), ())), preferred_element_type=f32)


def attend_kernel(
    ids, lengths_hbm, routes_hbm, route_weights_hbm, tokens_hbm, mix_hbm, head_gain_hbm, attn_gain_hbm, ffn_gain_hbm,
    query_hbm, key_hbm, value_hbm, cache_keys, cache_values, out_hbm,
    gate_hbm, up_hbm,
    pair, hidden, key_out, value_out, w_own, w_rest,
    query_w, key_w, value_w, keys, values, out_w, sem, query_rows, head_rows,
    lengths, routes, route_weights, tokens, mix_lambda, head_gain, attn_gain, ffn_gain, key_new, value_new,
):
    span = keys.shape[0] // 4
    copies = []

    def fetch(source, target):
        copies.append(pltpu.make_async_copy(source, target, sem.at[len(copies)]))
        copies[-1].start()
        return copies[-1]

    on_tokens = [fetch(tokens_hbm, tokens), fetch(attn_gain_hbm, attn_gain)]
    on_query = [fetch(query_hbm.at[pl.ds(k * 512, 512), :], query_w.at[pl.ds(k * 512, 512), :]) for k in range(4)]
    on_key = fetch(key_hbm, key_w)
    on_value = fetch(value_hbm, value_w)
    on_small = [
        fetch(lengths_hbm, lengths), fetch(mix_hbm, mix_lambda), fetch(head_gain_hbm, head_gain), fetch(ffn_gain_hbm, ffn_gain),
        fetch(routes_hbm, routes), fetch(route_weights_hbm, route_weights),
    ]
    on_keys, on_values = [], []
    for s in range(4):
        on_keys.append(fetch(cache_keys.at[pl.ds(s * span, span), :], keys.at[pl.ds(s * span, span), :]))
    for s in range(4):
        on_values.append(fetch(cache_values.at[pl.ds(s * span, span), :], values.at[pl.ds(s * span, span), :]))
    on_out = [fetch(out_hbm.at[pl.ds(k * 256, 256), :], out_w.at[pl.ds(k * 256, 256), :]) for k in range(4)]

    wide = gate_hbm.shape[1]
    ahead = []
    for half, target in ((ids[0], w_own), (1 - ids[0], w_rest)):
        rows = pl.ds(pl.multiple_of(half * HALF, HALF), HALF)
        ahead.append(fetch(gate_hbm.at[rows, :], target.at[:, pl.ds(0, wide)]))
        ahead.append(fetch(up_hbm.at[rows, :], target.at[:, pl.ds(wide, wide)]))
    for copy in on_tokens:
        copy.wait()
    x = tokens[...].astype(f32)
    normed = rms_norm(x, attn_gain[...], 1e-06).astype(bf16)
    query = None
    for k in range(4):
        on_query[k].wait()
        term = dot(normed[:, k * 512 : (k + 1) * 512], query_w[k * 512 : (k + 1) * 512, :])
        query = term if query is None else query + term
    query = query.astype(bf16).astype(f32)
    for s in range(4):
        for h in range(HEADS):
            query_rows[s * 8 + h : s * 8 + h + 1, :] = query[s : s + 1, h * HEAD_DIM : (h + 1) * HEAD_DIM]
    for copy in on_small:
        copy.wait()
    lane = lax.broadcasted_iota(jnp.int32, (4, TAIL), 1)
    row = lax.broadcasted_iota(jnp.int32, (4, TAIL), 0)
    tail = jnp.zeros((4, TAIL), f32)
    for t in range(4):
        for k in range(2):
            weight = jnp.full((4, TAIL), route_weights[k, t], f32)
            upper = weight.astype(bf16).astype(f32)
            there = row == t
            tail = jnp.where(there & (lane == routes[k, t]), upper, tail)
            tail = jnp.where(there & (lane == routes[k, t] + 8), weight - upper, tail)
    for half in range(2):
        pair[half, :, HALF:] = tail.astype(bf16)
    on_key.wait()
    knew = dot(normed, key_w[...]).astype(bf16)
    key_new[...] = knew
    written = [fetch(key_new, key_out)]
    on_value.wait()
    vnew = dot(normed, value_w[...]).astype(bf16)
    value_new[...] = vnew
    written.append(fetch(value_new, value_out))
    knew = knew.astype(f32)
    vnew = vnew.astype(f32)
    first = lax.broadcasted_iota(jnp.int32, (8, HEAD_DIM), 1) < HEAD_DIM // 2
    low_head = lax.broadcasted_iota(jnp.int32, (8, HEAD_DIM), 0) < 4
    lane = lax.broadcasted_iota(jnp.int32, (16, span), 1)
    row = lax.broadcasted_iota(jnp.int32, (16, span), 0)
    own_head = (lane & 1) == ((row >> 2) & 1)
    place = lane >> 1
    scale = (HEAD_DIM // 2) ** (-0.5)
    weights, own_weights = [], []
    lam = jnp.zeros((8, 1), f32)
    head = lax.broadcasted_iota(jnp.int32, (8, 1), 0)
    for h in range(HEADS):
        lam = jnp.where(head == h, mix_lambda[h], lam)
    for s in range(4):
        q = query_rows[s * 8 : s * 8 + 8, :]
        q = jnp.concatenate([jnp.where(first, q, 0.0), jnp.where(first, 0.0, q)])
        k_own = jnp.where(low_head, knew[s : s + 1, 0:HEAD_DIM], knew[s : s + 1, HEAD_DIM:])
        own = jnp.sum(q * jnp.concatenate([k_own, k_own]), axis=1, keepdims=True) * scale
        on_keys[s].wait()
        scores = dot_last(q.astype(bf16), keys[s * span : (s + 1) * span, :]) * scale
        scores = jnp.where(own_head & (place < lengths[s]), scores, -jnp.inf)
        largest = jnp.maximum(jnp.max(scores, axis=1, keepdims=True), own)
        raised = jnp.exp(scores - largest)
        own_raised = jnp.exp(own - largest)
        total = jnp.sum(raised, axis=1, keepdims=True) + own_raised
        prob = raised / total
        own_prob = own_raised / total
        weights.append((prob[0:8] - lam * prob[8:16]).astype(bf16))
        own_weights.append((own_prob[0:8] - lam * own_prob[8:16]).astype(bf16).astype(f32))
    for s in range(4):
        v_own = jnp.where(low_head, vnew[s : s + 1, 0:HEAD_DIM], vnew[s : s + 1, HEAD_DIM:])
        on_values[s].wait()
        mixed = dot(weights[s], values[s * span : (s + 1) * span, :]) + own_weights[s] * v_own
        heads = rms_norm(mixed, head_gain[...], 1e-05)
        for h in range(HEADS):
            head_rows[s : s + 1, h * HEAD_DIM : (h + 1) * HEAD_DIM] = heads[h : h + 1, :]
    heads = head_rows[...].astype(bf16)
    state = x
    for k in range(4):
        on_out[k].wait()
        state = state + dot(heads[:, k * 256 : (k + 1) * 256], out_w[k * 256 : (k + 1) * 256, :])
    hidden[...] = state
    ffn_in = rms_norm(state, ffn_gain[...], 1e-06).astype(bf16)
    for half in range(2):
        pair[half, :, 0:HALF] = ffn_in[:, half * HALF : (half + 1) * HALF]
    for copy in written + ahead:
        copy.wait()


def pieces_kernel(ids, gate, up, down, *refs):
    outs, held, sem = refs[:4], refs[4], refs[5]
    copies = [
        pltpu.make_async_copy(ref, held.at[m, pl.ds(0, ref.shape[0]), :], sem.at[m]) for m, ref in enumerate((gate, up, down))
    ]
    for copy in copies:
        copy.start()
    held[:, gate.shape[0] :, :] = jnp.zeros((3, 8 * UNITS - gate.shape[0], 256), bf16)
    for m in range(3):
        copies[m].wait()
        for k in range(4):
            for side in range(2):
                run = 2 * jnp.bitwise_and(ids[3] + k, 3) + jnp.bitwise_xor(ids[2], side)
                start = pl.multiple_of(run * UNITS, 16)
                at = side * PIECE + m * UNITS
                outs[k][at : at + UNITS, :] = held[m, pl.ds(start, UNITS), :]


def dot(a, b):
    return jnp.dot(a, b, preferred_element_type=f32)


def dense_sums(x, near, first):
    both = None
    for j in range(4):
        term = dot_last(x[:, j * 256 : (j + 1) * 256], near[first + j])
        both = term if both is None else both + term
    return both


def near_kernel(ids, own, first, second, third, fourth, crossed, branch, w_own, w_down, sums, both, near, w_out, sem):
    core = ids[0]
    wide = w_down.shape[0]
    copy = pltpu.make_async_copy(w_down, w_out.at[pl.ds(0, wide), :], sem)
    copy.start()
    near[...] = jnp.zeros_like(near)
    w_out[wide + UNITS :, :] = jnp.zeros((128 - UNITS, D), bf16)
    for b in range(8):
        near[b, 64:72, :] = jnp.broadcast_to(branch[:, b * 256 : (b + 1) * 256], (8, 256))
    for k, ref in enumerate((first, second, third, fourth)):
        for side in range(2):
            block = 2 * jnp.bitwise_and(ids[3] + 4 - k, 3) + jnp.bitwise_xor(ids[2], side)
            piece = ref[0:PIECE, :] if side == 0 else crossed[k]
            near[block, 0:UNITS, :] = piece[0:UNITS, :]
            near[block, 128 : 128 + UNITS, :] = piece[UNITS : 2 * UNITS, :]
            w_out[wide : wide + UNITS, pl.ds(pl.multiple_of(block * 256, 256), 256)] = piece[2 * UNITS :, :]
    x = own[:, :, 0:HALF].reshape(512, HALF)
    both[...] = dense_sums(x, near, core * 4)
    sums[...] = dot(x, w_own[...])
    copy.wait()


def rest_kernel(ids, theirs, sums_near, both_near, near, w_rest, w_out, y_other, acts):
    core, expert = ids[0], ids[1]
    x = theirs[:, :, 0:HALF].reshape(512, HALF)
    both = dense_sums(x, near, (1 - core) * 4) + both_near[...]
    sums = dot(x, w_rest[...]) + sums_near[...]
    wide = sums.shape[1] // 2
    gate_sum, up_sum = sums[:, 0:wide], sums[:, wide:]
    dense_gate = both[:, 0:128]
    lane = lax.broadcasted_iota(jnp.int32, (512, 128), 1)
    gate = jax.nn.sigmoid(jnp.sum(jnp.where(lane == 64, dense_gate, 0.0), axis=1, keepdims=True))
    tail = theirs[:, :, HALF : HALF + TAIL].reshape(512, TAIL).astype(f32)
    weight = jnp.sum(jnp.where((lane == expert) | (lane == expert + 8), tail, 0.0), axis=1, keepdims=True)
    dense_act = gate * (dense_gate * jax.nn.sigmoid(dense_gate) * both[:, 128:256])
    acts[:, 0:wide] = (weight * (gate_sum * jax.nn.sigmoid(gate_sum) * up_sum)).astype(bf16)
    acts[:, wide:] = jnp.where(lane < UNITS, dense_act, 0.0).astype(bf16)
    columns = pl.ds(pl.multiple_of((1 - core) * HALF, HALF), HALF)
    y_other[...] = dot(acts[...], w_out[:, columns]).astype(bf16)


def own_kernel(ids, acts, w_out, y_own):
    y_own[...] = dot(acts[...], w_out[:, pl.ds(pl.multiple_of(ids[0] * HALF, HALF), HALF)])


def join_kernel(y_own, y_recv, out):
    out[...] = (y_own[...] + y_recv[...].astype(f32)).astype(bf16).reshape(128, 4, HALF)


def last_kernel(hidden, parts, out):
    for half in range(2):
        total = jnp.zeros((4, HALF), f32)
        for chip in range(64):
            total = total + parts[2 * chip + half].astype(f32)
        cols = slice(half * HALF, (half + 1) * HALF)
        out[:, cols] = (hidden[:, cols] + total).astype(bf16)


def call(kernel, outs, operands, scratch=(), spaces=None):
    spaces = spaces or {}
    operands = [pltpu.with_memory_space_constraint(x, pltpu.HBM) if spaces.get(k) is pltpu.HBM else x for k, x in enumerate(operands)]
    return pl.pallas_call(
        kernel,
        in_specs=[pl.BlockSpec(memory_space=spaces.get(k, pltpu.VMEM)) for k in range(len(operands))],
        out_specs=[pl.BlockSpec(memory_space=space or pltpu.VMEM) for _, _, space in outs],
        out_shape=[space(shape, kind) if space else jax.ShapeDtypeStruct(shape, kind) for shape, kind, space in outs],
        scratch_shapes=list(scratch),
        compiler_params=pltpu.CompilerParams(vmem_limit_bytes=36 * 1024 * 1024),
    )(*operands)


def per_device(
    tokens, lengths, cache_keys, cache_values, query_w, key_w, value_w, out_w, mix_lambda, head_gain, attn_gain, ffn_gain,
    routes, route_weights, exp_gate, exp_up, exp_down, dense_gate, dense_up, dense_down, branch_gate,
):
    rows = tokens.shape[0]
    hidden_units = exp_gate.shape[1]
    me = lax.axis_index("ep")
    core = me % 2
    ids = jnp.stack([core, me // 16, me // 16 % 2, me // 32]).astype(jnp.int32)

    smem, hbm, vmem = pltpu.SMEM, pltpu.HBM, pltpu.VMEM
    pieces = call(
        pieces_kernel,
        [((2 * PIECE, 256), bf16, vmem)] * 4,
        [ids, jnp.swapaxes(dense_gate[0], 0, 1), jnp.swapaxes(dense_up[0], 0, 1), dense_down[0]],
        [pltpu.VMEM((3, 8 * UNITS, 256), bf16), pltpu.SemaphoreType.DMA((3,))],
        {0: smem, 1: hbm, 2: hbm, 3: hbm},
    )
    turned = [lax.ppermute(pieces[k], "ep", [(i, (i + 32 * k) % DEVICES) for i in range(DEVICES)]) for k in (1, 3, 2)]
    pieces = [pieces[0], turned[0], turned[2], turned[1]]

    positions = cache_keys.shape[0] * cache_keys.shape[1] * KV_HEADS
    pair, hidden_state, key_new, value_new, w_own, w_rest = call(
        attend_kernel,
        [
            ((2, rows, HALF + TAIL), bf16, vmem), ((rows, D), f32, vmem),
            ((rows, KV_HEADS * HEAD_DIM), bf16, hbm), ((rows, KV_HEADS * HEAD_DIM), bf16, hbm),
            ((HALF, 2 * hidden_units), bf16, vmem), ((HALF, 2 * hidden_units), bf16, vmem),
        ],
        [
            ids, lengths, routes.T, route_weights.T, tokens, mix_lambda, head_gain.reshape(1, HEAD_DIM),
            attn_gain.reshape(1, D), ffn_gain.reshape(1, D), query_w, key_w, value_w,
            cache_keys.reshape(positions, HEAD_DIM), cache_values.reshape(positions, HEAD_DIM), out_w, exp_gate, exp_up,
        ],
        [
            pltpu.VMEM(query_w.shape, bf16), pltpu.VMEM(key_w.shape, bf16), pltpu.VMEM(value_w.shape, bf16),
            pltpu.VMEM((positions, HEAD_DIM), bf16), pltpu.VMEM((positions, HEAD_DIM), bf16), pltpu.VMEM(out_w.shape, bf16),
            pltpu.SemaphoreType.DMA((32,)), pltpu.VMEM((32, HEAD_DIM), f32), pltpu.VMEM((rows, HEADS * HEAD_DIM), f32),
            pltpu.SMEM((rows,), jnp.int32), pltpu.SMEM((2, rows), jnp.int32), pltpu.SMEM((2, rows), f32), pltpu.VMEM((rows, D), bf16),
            pltpu.SMEM((HEADS,), f32), pltpu.VMEM((1, HEAD_DIM), f32), pltpu.VMEM((1, D), f32), pltpu.VMEM((1, D), f32),
            pltpu.VMEM((rows, KV_HEADS * HEAD_DIM), bf16), pltpu.VMEM((rows, KV_HEADS * HEAD_DIM), bf16),
        ],
        {0: smem, **{k: hbm for k in range(1, 17)}},
    )
    outgoing = jnp.broadcast_to(pair[None], (64, 2, rows, HALF + TAIL)).reshape(DEVICES, rows, HALF + TAIL)
    crossed = lax.ppermute(jnp.stack([x[PIECE:] for x in pieces]), "ep", [(i, i ^ 16) for i in range(DEVICES)])
    own = lax.all_to_all(outgoing, "ep", 0, 0, tiled=True)
    theirs = to_partner(own)
    sums, both, near, w_out = call(
        near_kernel,
        [
            ((512, 2 * hidden_units), f32, vmem), ((512, 256), f32, vmem), ((8, 256, 256), bf16, vmem),
            ((hidden_units + 128, D), bf16, vmem),
        ],
        [ids, own, *pieces, crossed, branch_gate.reshape(1, D), w_own, exp_down],
        [pltpu.SemaphoreType.DMA],
        {0: smem, 9: hbm},
    )
    y_other, acts = call(
        rest_kernel,
        [((512, HALF), bf16, vmem), ((512, hidden_units + 128), bf16, vmem)],
        [ids, theirs, sums, both, near, w_rest, w_out],
        [],
        {0: smem},
    )
    y_recv = to_partner(y_other)
    (y_own,) = call(own_kernel, [((512, HALF), f32, vmem)], [ids, acts, w_out], [], {0: smem})
    (joined,) = call(join_kernel, [((DEVICES, rows, HALF), bf16, vmem)], [y_own, y_recv])
    parts = lax.all_to_all(joined, "ep", 0, 0, tiled=True)
    (output,) = call(last_kernel, [((rows, D), bf16, None)], [hidden_state, parts])
    return (output, key_new, value_new)


def solution(mesh):
    placed = (
        P("ep", None),
        P("ep"),
        P("ep", None, None, None),
        P("ep", None, None, None),
        P(),
        P(),
        P(),
        P(),
        P(),
        P(),
        P(),
        P(),
        P("ep", None),
        P("ep", None),
        P(None, "ep"),
        P(None, "ep"),
        P("ep", None),
        P("ep", None, None),
        P("ep", None, None),
        P("ep", None, None),
        P(),
    )

    return jax.shard_map(
        per_device,
        mesh=mesh,
        in_specs=placed,
        out_specs=(P("ep", None), P("ep", None), P("ep", None)),
        check_vma=False,
    )
```

```python
import jax
import jax.numpy as jnp
from jax import lax
from jax.experimental import pallas as pl
from jax.experimental.pallas import tpu as pltpu
from jax.sharding import PartitionSpec as P


HEADS = 8
KV_HEADS = 2
HEAD_DIM = 128
DEVICES = 128
D = 2048
HALF = D // 2
UNITS = 48
PIECE = 3 * UNITS
TAIL = 128
f32 = jnp.float32
bf16 = jnp.bfloat16


def to_partner(x):
    return lax.ppermute(x, "ep", [(i, i ^ 1) for i in range(DEVICES)])


def rms_norm(values, gain, epsilon):
    scale = lax.rsqrt(jnp.mean(values * values, axis=-1, keepdims=True) + epsilon)
    return values * scale * gain


def dot_last(a, b):
    return lax.dot_general(a, b, (((1,), (1,)), ((), ())), preferred_element_type=f32)


def attend_kernel(
    ids, lengths_hbm, routes_hbm, route_weights_hbm, tokens_hbm, mix_hbm, head_gain_hbm, attn_gain_hbm, ffn_gain_hbm,
    query_hbm, key_hbm, value_hbm, cache_keys, cache_values, out_hbm,
    gate_hbm, up_hbm, down_hbm,
    pair, hidden, key_out, value_out, w_own, w_rest, w_down,
    query_w, key_w, value_w, keys, values, out_w, sem, query_rows, head_rows,
    lengths, routes, route_weights, tokens, mix_lambda, head_gain, attn_gain, ffn_gain, key_new, value_new,
):
    span = keys.shape[0] // 4
    copies = []

    def fetch(source, target):
        copies.append(pltpu.make_async_copy(source, target, sem.at[len(copies)]))
        copies[-1].start()
        return copies[-1]

    on_tokens = [fetch(tokens_hbm, tokens), fetch(attn_gain_hbm, attn_gain)]
    on_query = [fetch(query_hbm.at[pl.ds(k * 512, 512), :], query_w.at[pl.ds(k * 512, 512), :]) for k in range(4)]
    on_key = fetch(key_hbm, key_w)
    on_value = fetch(value_hbm, value_w)
    on_small = [
        fetch(lengths_hbm, lengths), fetch(mix_hbm, mix_lambda), fetch(head_gain_hbm, head_gain), fetch(ffn_gain_hbm, ffn_gain),
        fetch(routes_hbm, routes), fetch(route_weights_hbm, route_weights),
    ]
    on_keys, on_values = [], []
    for s in range(4):
        on_keys.append(fetch(cache_keys.at[pl.ds(s * span, span), :], keys.at[pl.ds(s * span, span), :]))
    for s in range(4):
        on_values.append(fetch(cache_values.at[pl.ds(s * span, span), :], values.at[pl.ds(s * span, span), :]))
    on_out = [fetch(out_hbm.at[pl.ds(k * 256, 256), :], out_w.at[pl.ds(k * 256, 256), :]) for k in range(4)]

    wide = gate_hbm.shape[1]
    ahead = [fetch(down_hbm, w_down)]
    for half, target in ((ids[0], w_own), (1 - ids[0], w_rest)):
        rows = pl.ds(pl.multiple_of(half * HALF, HALF), HALF)
        ahead.append(fetch(gate_hbm.at[rows, :], target.at[:, pl.ds(0, wide)]))
        ahead.append(fetch(up_hbm.at[rows, :], target.at[:, pl.ds(wide, wide)]))
    for copy in on_tokens:
        copy.wait()
    x = tokens[...].astype(f32)
    normed = rms_norm(x, attn_gain[...], 1e-06).astype(bf16)
    query = None
    for k in range(4):
        on_query[k].wait()
        term = dot(normed[:, k * 512 : (k + 1) * 512], query_w[k * 512 : (k + 1) * 512, :])
        query = term if query is None else query + term
    query = query.astype(bf16).astype(f32)
    for s in range(4):
        for h in range(HEADS):
            query_rows[s * 8 + h : s * 8 + h + 1, :] = query[s : s + 1, h * HEAD_DIM : (h + 1) * HEAD_DIM]
    for copy in on_small:
        copy.wait()
    lane = lax.broadcasted_iota(jnp.int32, (4, TAIL), 1)
    row = lax.broadcasted_iota(jnp.int32, (4, TAIL), 0)
    tail = jnp.zeros((4, TAIL), f32)
    for t in range(4):
        for k in range(2):
            weight = jnp.full((4, TAIL), route_weights[k, t], f32)
            upper = weight.astype(bf16).astype(f32)
            there = row == t
            tail = jnp.where(there & (lane == routes[k, t]), upper, tail)
            tail = jnp.where(there & (lane == routes[k, t] + 8), weight - upper, tail)
    for half in range(2):
        pair[half, :, HALF:] = tail.astype(bf16)
    on_key.wait()
    knew = dot(normed, key_w[...]).astype(bf16)
    key_new[...] = knew
    written = [fetch(key_new, key_out)]
    on_value.wait()
    vnew = dot(normed, value_w[...]).astype(bf16)
    value_new[...] = vnew
    written.append(fetch(value_new, value_out))
    knew = knew.astype(f32)
    vnew = vnew.astype(f32)
    first = lax.broadcasted_iota(jnp.int32, (8, HEAD_DIM), 1) < HEAD_DIM // 2
    low_head = lax.broadcasted_iota(jnp.int32, (8, HEAD_DIM), 0) < 4
    lane = lax.broadcasted_iota(jnp.int32, (16, span), 1)
    row = lax.broadcasted_iota(jnp.int32, (16, span), 0)
    own_head = (lane & 1) == ((row >> 2) & 1)
    place = lane >> 1
    scale = (HEAD_DIM // 2) ** (-0.5)
    weights, own_weights = [], []
    lam = jnp.zeros((8, 1), f32)
    head = lax.broadcasted_iota(jnp.int32, (8, 1), 0)
    for h in range(HEADS):
        lam = jnp.where(head == h, mix_lambda[h], lam)
    for s in range(4):
        q = query_rows[s * 8 : s * 8 + 8, :]
        q = jnp.concatenate([jnp.where(first, q, 0.0), jnp.where(first, 0.0, q)])
        k_own = jnp.where(low_head, knew[s : s + 1, 0:HEAD_DIM], knew[s : s + 1, HEAD_DIM:])
        own = jnp.sum(q * jnp.concatenate([k_own, k_own]), axis=1, keepdims=True) * scale
        on_keys[s].wait()
        scores = dot_last(q.astype(bf16), keys[s * span : (s + 1) * span, :]) * scale
        scores = jnp.where(own_head & (place < lengths[s]), scores, -jnp.inf)
        largest = jnp.maximum(jnp.max(scores, axis=1, keepdims=True), own)
        raised = jnp.exp(scores - largest)
        own_raised = jnp.exp(own - largest)
        total = jnp.sum(raised, axis=1, keepdims=True) + own_raised
        prob = raised / total
        own_prob = own_raised / total
        weights.append((prob[0:8] - lam * prob[8:16]).astype(bf16))
        own_weights.append((own_prob[0:8] - lam * own_prob[8:16]).astype(bf16).astype(f32))
    for s in range(4):
        v_own = jnp.where(low_head, vnew[s : s + 1, 0:HEAD_DIM], vnew[s : s + 1, HEAD_DIM:])
        on_values[s].wait()
        mixed = dot(weights[s], values[s * span : (s + 1) * span, :]) + own_weights[s] * v_own
        heads = rms_norm(mixed, head_gain[...], 1e-05)
        for h in range(HEADS):
            head_rows[s : s + 1, h * HEAD_DIM : (h + 1) * HEAD_DIM] = heads[h : h + 1, :]
    heads = head_rows[...].astype(bf16)
    state = x
    for k in range(4):
        on_out[k].wait()
        state = state + dot(heads[:, k * 256 : (k + 1) * 256], out_w[k * 256 : (k + 1) * 256, :])
    hidden[...] = state
    ffn_in = rms_norm(state, ffn_gain[...], 1e-06).astype(bf16)
    for half in range(2):
        pair[half, :, 0:HALF] = ffn_in[:, half * HALF : (half + 1) * HALF]
    for copy in written + ahead:
        copy.wait()


def pieces_kernel(ids, gate, up, down, *refs):
    outs, held, sem = refs[:4], refs[4], refs[5]
    copies = [
        pltpu.make_async_copy(ref, held.at[m, pl.ds(0, ref.shape[0]), :], sem.at[m]) for m, ref in enumerate((gate, up, down))
    ]
    for copy in copies:
        copy.start()
    held[:, gate.shape[0] :, :] = jnp.zeros((3, 8 * UNITS - gate.shape[0], 256), bf16)
    for m in range(3):
        copies[m].wait()
        for k in range(4):
            for side in range(2):
                run = 2 * jnp.bitwise_and(ids[3] + k, 3) + jnp.bitwise_xor(ids[2], side)
                start = pl.multiple_of(run * UNITS, 16)
                at = side * PIECE + m * UNITS
                outs[k][at : at + UNITS, :] = held[m, pl.ds(start, UNITS), :]


def dot(a, b):
    return jnp.dot(a, b, preferred_element_type=f32)


def dense_sums(x, near, first):
    both = None
    for j in range(4):
        term = dot_last(x[:, j * 256 : (j + 1) * 256], near[first + j])
        both = term if both is None else both + term
    return both


def near_kernel(ids, own, first, second, third, fourth, crossed, branch, w_own, w_down, sums, both, near, w_out, sem):
    core = ids[0]
    wide = w_down.shape[0]
    copy = pltpu.make_async_copy(w_down, w_out.at[pl.ds(0, wide), :], sem)
    copy.start()
    near[...] = jnp.zeros_like(near)
    w_out[wide + UNITS :, :] = jnp.zeros((128 - UNITS, D), bf16)
    for b in range(8):
        near[b, 64:72, :] = jnp.broadcast_to(branch[:, b * 256 : (b + 1) * 256], (8, 256))
    for k, ref in enumerate((first, second, third, fourth)):
        for side in range(2):
            block = 2 * jnp.bitwise_and(ids[3] + 4 - k, 3) + jnp.bitwise_xor(ids[2], side)
            piece = ref[0:PIECE, :] if side == 0 else crossed[k]
            near[block, 0:UNITS, :] = piece[0:UNITS, :]
            near[block, 128 : 128 + UNITS, :] = piece[UNITS : 2 * UNITS, :]
            w_out[wide : wide + UNITS, pl.ds(pl.multiple_of(block * 256, 256), 256)] = piece[2 * UNITS :, :]
    x = own[:, :, 0:HALF].reshape(512, HALF)
    both[...] = dense_sums(x, near, core * 4)
    sums[...] = dot(x, w_own[...])
    copy.wait()


def rest_kernel(ids, theirs, sums_near, both_near, near, w_rest, w_out, y_first, y_second, acts):
    core, expert = ids[0], ids[1]
    x = theirs[:, :, 0:HALF].reshape(512, HALF)
    both = dense_sums(x, near, (1 - core) * 4) + both_near[...]
    sums = dot(x, w_rest[...]) + sums_near[...]
    wide = sums.shape[1] // 2
    gate_sum, up_sum = sums[:, 0:wide], sums[:, wide:]
    dense_gate = both[:, 0:128]
    lane = lax.broadcasted_iota(jnp.int32, (512, 128), 1)
    gate = jax.nn.sigmoid(jnp.sum(jnp.where(lane == 64, dense_gate, 0.0), axis=1, keepdims=True))
    tail = theirs[:, :, HALF : HALF + TAIL].reshape(512, TAIL).astype(f32)
    weight = jnp.sum(jnp.where((lane == expert) | (lane == expert + 8), tail, 0.0), axis=1, keepdims=True)
    dense_act = gate * (dense_gate * jax.nn.sigmoid(dense_gate) * both[:, 128:256])
    acts[:, 0:wide] = (weight * (gate_sum * jax.nn.sigmoid(gate_sum) * up_sum)).astype(bf16)
    acts[:, wide:] = jnp.where(lane < UNITS, dense_act, 0.0).astype(bf16)
    columns = pl.ds(pl.multiple_of((1 - core) * HALF, HALF), HALF)
    total = dot(acts[...], w_out[:, columns]).astype(bf16)
    y_first[...] = total[:, 0 : HALF // 2]
    y_second[...] = total[:, HALF // 2 :]


def own_kernel(ids, acts, w_out, y_own):
    y_own[...] = dot(acts[...], w_out[:, pl.ds(pl.multiple_of(ids[0] * HALF, HALF), HALF)])


def join_kernel(y_own, first, second, out):
    wide = first.shape[1]
    for k, ref in enumerate((first, second)):
        columns = slice(k * wide, (k + 1) * wide)
        out[:, :, columns] = (y_own[:, columns] + ref[...].astype(f32)).astype(bf16).reshape(128, 4, wide)


def last_kernel(hidden, parts, out):
    for half in range(2):
        total = jnp.zeros((4, HALF), f32)
        for chip in range(64):
            total = total + parts[2 * chip + half].astype(f32)
        cols = slice(half * HALF, (half + 1) * HALF)
        out[:, cols] = (hidden[:, cols] + total).astype(bf16)


def call(kernel, outs, operands, scratch=(), spaces=None):
    spaces = spaces or {}
    operands = [pltpu.with_memory_space_constraint(x, pltpu.HBM) if spaces.get(k) is pltpu.HBM else x for k, x in enumerate(operands)]
    return pl.pallas_call(
        kernel,
        in_specs=[pl.BlockSpec(memory_space=spaces.get(k, pltpu.VMEM)) for k in range(len(operands))],
        out_specs=[pl.BlockSpec(memory_space=space or pltpu.VMEM) for _, _, space in outs],
        out_shape=[space(shape, kind) if space else jax.ShapeDtypeStruct(shape, kind) for shape, kind, space in outs],
        scratch_shapes=list(scratch),
        compiler_params=pltpu.CompilerParams(vmem_limit_bytes=36 * 1024 * 1024),
    )(*operands)


def per_device(
    tokens, lengths, cache_keys, cache_values, query_w, key_w, value_w, out_w, mix_lambda, head_gain, attn_gain, ffn_gain,
    routes, route_weights, exp_gate, exp_up, exp_down, dense_gate, dense_up, dense_down, branch_gate,
):
    rows = tokens.shape[0]
    hidden_units = exp_gate.shape[1]
    me = lax.axis_index("ep")
    core = me % 2
    ids = jnp.stack([core, me // 16, me // 16 % 2, me // 32]).astype(jnp.int32)

    smem, hbm, vmem = pltpu.SMEM, pltpu.HBM, pltpu.VMEM
    pieces = call(
        pieces_kernel,
        [((2 * PIECE, 256), bf16, vmem)] * 4,
        [ids, jnp.swapaxes(dense_gate[0], 0, 1), jnp.swapaxes(dense_up[0], 0, 1), dense_down[0]],
        [pltpu.VMEM((3, 8 * UNITS, 256), bf16), pltpu.SemaphoreType.DMA((3,))],
        {0: smem, 1: hbm, 2: hbm, 3: hbm},
    )
    turned = [lax.ppermute(pieces[k], "ep", [(i, (i + 32 * k) % DEVICES) for i in range(DEVICES)]) for k in (1, 3, 2)]
    pieces = [pieces[0], turned[0], turned[2], turned[1]]

    positions = cache_keys.shape[0] * cache_keys.shape[1] * KV_HEADS
    pair, hidden_state, key_new, value_new, w_own, w_rest, w_down = call(
        attend_kernel,
        [
            ((2, rows, HALF + TAIL), bf16, vmem), ((rows, D), f32, vmem),
            ((rows, KV_HEADS * HEAD_DIM), bf16, hbm), ((rows, KV_HEADS * HEAD_DIM), bf16, hbm),
            ((HALF, 2 * hidden_units), bf16, vmem), ((HALF, 2 * hidden_units), bf16, vmem), (exp_down.shape, bf16, vmem),
        ],
        [
            ids, lengths, routes.T, route_weights.T, tokens, mix_lambda, head_gain.reshape(1, HEAD_DIM),
            attn_gain.reshape(1, D), ffn_gain.reshape(1, D), query_w, key_w, value_w,
            cache_keys.reshape(positions, HEAD_DIM), cache_values.reshape(positions, HEAD_DIM), out_w, exp_gate, exp_up, exp_down,
        ],
        [
            pltpu.VMEM(query_w.shape, bf16), pltpu.VMEM(key_w.shape, bf16), pltpu.VMEM(value_w.shape, bf16),
            pltpu.VMEM((positions, HEAD_DIM), bf16), pltpu.VMEM((positions, HEAD_DIM), bf16), pltpu.VMEM(out_w.shape, bf16),
            pltpu.SemaphoreType.DMA((33,)), pltpu.VMEM((32, HEAD_DIM), f32), pltpu.VMEM((rows, HEADS * HEAD_DIM), f32),
            pltpu.SMEM((rows,), jnp.int32), pltpu.SMEM((2, rows), jnp.int32), pltpu.SMEM((2, rows), f32), pltpu.VMEM((rows, D), bf16),
            pltpu.SMEM((HEADS,), f32), pltpu.VMEM((1, HEAD_DIM), f32), pltpu.VMEM((1, D), f32), pltpu.VMEM((1, D), f32),
            pltpu.VMEM((rows, KV_HEADS * HEAD_DIM), bf16), pltpu.VMEM((rows, KV_HEADS * HEAD_DIM), bf16),
        ],
        {0: smem, **{k: hbm for k in range(1, 18)}},
    )
    outgoing = jnp.broadcast_to(pair[None], (64, 2, rows, HALF + TAIL)).reshape(DEVICES, rows, HALF + TAIL)
    crossed = lax.ppermute(jnp.stack([x[PIECE:] for x in pieces]), "ep", [(i, i ^ 16) for i in range(DEVICES)])
    own = lax.all_to_all(outgoing, "ep", 0, 0, tiled=True)
    theirs = to_partner(own)
    sums, both, near, w_out = call(
        near_kernel,
        [
            ((512, 2 * hidden_units), f32, vmem), ((512, 256), f32, vmem), ((8, 256, 256), bf16, vmem),
            ((hidden_units + 128, D), bf16, vmem),
        ],
        [ids, own, *pieces, crossed, branch_gate.reshape(1, D), w_own, w_down],
        [pltpu.SemaphoreType.DMA],
        {0: smem},
    )
    y_first, y_second, acts = call(
        rest_kernel,
        [((512, HALF // 2), bf16, vmem), ((512, HALF // 2), bf16, vmem), ((512, hidden_units + 128), bf16, vmem)],
        [ids, theirs, sums, both, near, w_rest, w_out],
        [],
        {0: smem},
    )
    y_recv = [to_partner(y_first), to_partner(y_second)]
    (y_own,) = call(own_kernel, [((512, HALF), f32, vmem)], [ids, acts, w_out], [], {0: smem})
    (joined,) = call(join_kernel, [((DEVICES, rows, HALF), bf16, vmem)], [y_own, *y_recv])
    parts = lax.all_to_all(joined, "ep", 0, 0, tiled=True)
    (output,) = call(last_kernel, [((rows, D), bf16, None)], [hidden_state, parts])
    return (output, key_new, value_new)


def solution(mesh):
    placed = (
        P("ep", None),
        P("ep"),
        P("ep", None, None, None),
        P("ep", None, None, None),
        P(),
        P(),
        P(),
        P(),
        P(),
        P(),
        P(),
        P(),
        P("ep", None),
        P("ep", None),
        P(None, "ep"),
        P(None, "ep"),
        P("ep", None),
        P("ep", None, None),
        P("ep", None, None),
        P("ep", None, None),
        P(),
    )

    return jax.shard_map(
        per_device,
        mesh=mesh,
        in_specs=placed,
        out_specs=(P("ep", None), P("ep", None), P("ep", None)),
        check_vma=False,
    )
```
